256 devices in a mesh: ep: 64 (over z, y, core), tp: 4 (over x).
Axes of the slice: x: 4, y: 4, z: 8, core: 2. Of those that a mesh axis runs over, the one named last changes fastest.
Arguments:
- glu_value: bfloat16 [32768, 1024], P('ep', 'tp'), may hold values from -6 to 6
- glu_gate: bfloat16 [32768, 1024], P('ep', 'tp'), may hold values from -12 to 12
- conv_kernel: float32 [31, 1024], P(None, 'tp'), may hold values from -11.49474 to 11.49474
- ln_gain: float32 [1024], P('tp'), may hold values from 0.1 to 1.9
- out_weight: bfloat16 [1024, 2048], P('tp'), may hold values from -0.1875 to 0.1875
- moe_input: bfloat16 [16384, 2048], P('ep'), may hold values from -6 to 6
- moe_gain: float32 [2048], replicated, may hold values from 0.1 to 1.9
- gate_weight: bfloat16 [64, 2048, 3072], P('ep', None, 'tp'), may hold values from -0.125 to 0.125
- up_weight: bfloat16 [64, 2048, 3072], P('ep', None, 'tp'), may hold values from -0.125 to 0.125
- down_weight: bfloat16 [64, 3072, 2048], P('ep', 'tp'), may hold values from -0.109375 to 0.109375
- expert_ids: int32 [16384, 2], P('ep'), may hold values from 0 to 63, all different within a row; in each aligned block of 256 rows (0 to 255, 256 to 511, ...) at most 16 rows name the same one
- route_weight: float32 [16384, 2], P('ep'), may hold values from 0.2 to 1
Outputs:
- mixer_out: bfloat16 [32768, 2048], P(('ep', 'tp'))
- expert_out: bfloat16 [16384, 2048], P('ep', 'tp')
The draws below stay inside these ranges and needn't reach their ends.
Inputs may be any that keep to these rules, and one draw needn't show every extreme that they name: `expert_ids`: each row names 2 different experts. In the rows of one device no expert is named by more than 16 rows; the bound is reached at some expert in some device's rows.
All inputs are finite; a program needn't handle non-finite values.
Results may differ from the reference program's by a relative error of at most 0.012.
Values may be sent and summed in bfloat16 or wider, within the bound.
A program may use at most 64 MiB of HBM per device.

```python
import math
import jax
import jax.numpy as jnp
import numpy as np
from jax import lax

D = 2048
MIX = 1024
KERNEL = 31
FF = 3072
TOP = 2
TOKB_DEV = 256
EXPERTS = 64
CAP = 16
TOKA = 32768
TOKB = 16384
N_EP = 64
N_TP = 4


def draw_conv_kernel(key, part):
    base_key = jax.random.fold_in(key, 17)
    rough_key = jax.random.fold_in(key, 29)
    position = jnp.arange(MIX, dtype=jnp.float32) / MIX
    rough = jnp.exp(jax.random.uniform(rough_key, (MIX,), jnp.float32, math.log(0.6), math.log(1.6)))
    scale = jnp.exp(position * math.log(10.0)) * rough * KERNEL ** (-0.5)
    base = jnp.clip(jax.random.normal(base_key, (KERNEL, MIX), jnp.float32), -4.0, 4.0)
    return (base * scale[None, :]).astype(jnp.float32)


def level_of(key, shape, shards, low, high):
    def one(axis_at, shards_of):
        heights = jax.random.uniform(jax.random.fold_in(jax.random.fold_in(key, 6), axis_at), (shards_of,), jnp.float32, low / len(shards), high / len(shards))
        return jnp.repeat(jnp.exp(heights), shape[axis_at] // shards_of).reshape((-1,) + (1,) * (len(shape) - axis_at - 1))

    level = one(*shards[0])
    for cut in shards[1:]:
        level = level * one(*cut)
    return level


def shared_out(key, own, number, rows, number_of, top, reach, skew):
    ranking = jax.random.permutation(key, number_of)
    crowded, ordinary = load_shares(number_of, rows * top, reach, skew, True), load_shares(number_of, rows * top, reach, skew, False)
    places = jnp.arange(number_of)

    def named(tallies, offset_by):
        used = int((tallies > 0).sum())
        fixed = max(1, used // 4)
        moved = fixed + (places - fixed + offset_by * (used - fixed)) % max(1, number_of - fixed)
        return jnp.zeros((number_of,), jnp.int32).at[ranking[jnp.where(places < fixed, places, moved)]].set(jnp.asarray(tallies, jnp.int32))

    tallies = jnp.where(number % 4 == 0, named(crowded, number // 4), named(ordinary, number - number // 4 - 1))
    mixed = jax.random.permutation(jax.random.fold_in(own, 3), number_of)
    donor, receiver = mixed[0:number_of // 2 * 2:2], mixed[1:number_of // 2 * 2:2]
    margin = jnp.minimum(tallies[donor] - 1, reach - tallies[receiver]) // 2
    margin = jnp.where((donor == ranking[0]) | (receiver == ranking[0]) | (tallies[receiver] == 0), 0, jnp.maximum(margin, 0))
    moved = jax.random.randint(jax.random.fold_in(own, 4), (number_of // 2,), 0, 1 << 20) % (margin + 1)
    tallies = tallies.at[donor].add(-moved).at[receiver].add(moved)
    members = jnp.searchsorted(jnp.cumsum(tallies), jnp.arange(rows * top), side="right").astype(jnp.int32)
    grid = members.reshape(top, rows).T
    grid = grid[jax.random.permutation(jax.random.fold_in(own, 1), rows)]
    offset_by = jax.random.randint(jax.random.fold_in(own, 2), (rows, 1), 0, top)
    return jnp.take_along_axis(grid, (jnp.arange(top)[None, :] + offset_by) % top, axis=1)


def load_shares(number_of, total, most, skew, full):
    portions = [(1 << 20) // math.isqrt(rank ** skew) + 1 for rank in range(1, number_of + 1)]
    largest = most if full else min(most, max(-(-total // number_of), total * portions[0] // sum(portions)))
    least = 1 if total - largest >= number_of - 1 else 0
    counts, rest = [largest] + [least] * (number_of - 1), total - largest - least * (number_of - 1)
    while rest > 0:
        movable = [i for i in range(1, number_of) if counts[i] < largest] or [i for i in range(1, number_of) if counts[i] < most]
        pool, budget = sum([portions[i] for i in movable]), rest
        for i in movable:
            extra = min(most - counts[i], max(1, budget * portions[i] // pool), rest)
            counts[i] = counts[i] + extra
            rest = rest - extra
    return np.array(counts)


def normal_values(key, shape, scale, limit, pieces=(), kind=jnp.bfloat16):
    entries = scale * jax.random.normal(key, shape, jnp.float32)
    if pieces:
        entries = entries * level_of(key, shape, pieces, -0.22, 0.18)
    return jnp.clip(entries, -limit, limit).astype(kind)


def setup_inputs(seed: int = 0) -> dict:
    streams_of = jax.random.split(jax.random.key(seed), 13)
    glu_value = normal_values(streams_of[0], (TOKA, MIX), 1.0, 6.0, ((0, 64), (1, 4)))
    glu_gate = normal_values(streams_of[1], (TOKA, MIX), 2.0, 12.0, ((0, 64), (1, 4)))
    conv_kernel = draw_conv_kernel(jax.random.fold_in(streams_of[12], 71), 0)
    ln_gain = jnp.clip(1.0 + 0.18 * jax.random.normal(streams_of[3], (MIX,), jnp.float32), 0.1, 1.9)
    out_weight = normal_values(streams_of[4], (MIX, D), MIX ** -0.5, 0.1875, ((0, 4),))
    moe_input = normal_values(streams_of[5], (TOKB, D), 1.0, 6.0, ((0, 64),))
    moe_gain = jnp.clip(1.0 + 0.18 * jax.random.normal(streams_of[6], (D,), jnp.float32), 0.1, 1.9)
    gate_weight = normal_values(streams_of[7], (EXPERTS, D, FF), D ** -0.5, 0.125, ((0, 64), (2, 4)))
    up_weight = normal_values(streams_of[8], (EXPERTS, D, FF), D ** -0.5, 0.125, ((0, 64), (2, 4)))
    down_weight = normal_values(streams_of[9], (EXPERTS, FF, D), FF ** -0.5, 0.109375, ((0, 64), (1, 4)))
    expert_ids_keys = jax.random.split(jax.random.fold_in(streams_of[10], 1), TOKB // TOKB_DEV)
    expert_ids_turns = jax.random.permutation(jax.random.fold_in(streams_of[10], 3), TOKB // TOKB_DEV)
    expert_ids = jax.vmap(lambda own, number: shared_out(jax.random.fold_in(streams_of[10], 2), own, number, TOKB_DEV, EXPERTS, TOP, CAP, 1))(expert_ids_keys, expert_ids_turns).reshape((TOKB, TOP))
    route_weight = jnp.clip(0.2 + 0.8 * jax.random.uniform(streams_of[11], (TOKB, TOP), jnp.float32) ** level_of(streams_of[11], (TOKB, TOP), ((0, 64),), -0.2, 0.2), 0.2, 1.0)
    return {"glu_value": glu_value, "glu_gate": glu_gate, "conv_kernel": conv_kernel, "ln_gain": ln_gain, "out_weight": out_weight, "moe_input": moe_input, "moe_gain": moe_gain, "gate_weight": gate_weight, "up_weight": up_weight, "down_weight": down_weight, "expert_ids": expert_ids, "route_weight": route_weight}


eps_rms = 1e-06
eps_norm = 1e-05

def slot_numbers(expert_ids, experts, capacity):
    chosen = expert_ids.reshape(-1)
    onehot = (chosen[:, None] == jnp.arange(experts, dtype=jnp.int32)[None, :]).astype(jnp.int32)
    earlier = jnp.cumsum(onehot, axis=0) - onehot
    position = lax.optimization_barrier(jnp.sum(earlier * onehot, axis=1))
    return (chosen * capacity + position).astype(jnp.int32)

def fill_slots(normed, slot_index, experts, capacity, chosen_per_token):
    owners = jnp.full((experts * capacity,), -1, jnp.int32)
    token_of = (jnp.arange(slot_index.shape[0], dtype=jnp.int32) // chosen_per_token).astype(jnp.int32)
    owners = owners.at[slot_index].set(token_of)
    picked = jnp.take(normed, jnp.maximum(owners, 0), axis=0)
    filled = jnp.where((owners >= 0)[:, None], picked, jnp.zeros_like(picked))
    return filled.reshape(experts, capacity, normed.shape[1])

def mixer_half(glu_value, glu_gate, conv_kernel, ln_gain, out_weight):
    gated = (glu_value.astype(jnp.float32) * jax.nn.sigmoid(glu_gate.astype(jnp.float32))).astype(jnp.bfloat16)
    length = gated.shape[0]
    padded = jnp.concatenate([jnp.zeros((KERNEL - 1, MIX), jnp.bfloat16), gated], axis=0).astype(jnp.float32)
    convolved = jnp.zeros((length, MIX), jnp.float32)
    for tap_index in range(KERNEL):
        begin = KERNEL - 1 - tap_index
        convolved = convolved + conv_kernel[tap_index] * padded[begin:begin + length]
    total = lax.optimization_barrier(jnp.sum(convolved, axis=1))
    squares = lax.optimization_barrier(jnp.sum(convolved * convolved, axis=1))
    mean = total / MIX
    variance = squares / MIX - mean * mean
    scaled = (convolved - mean[:, None]) * lax.rsqrt(variance + eps_norm)[:, None] * ln_gain
    activated = jax.nn.silu(scaled).astype(jnp.bfloat16)
    group = MIX // N_TP
    result = jnp.zeros((length, D), jnp.float32)
    for part_index in range(N_TP):
        partial_sum = jnp.dot(activated[:, part_index * group:(part_index + 1) * group], out_weight[part_index * group:(part_index + 1) * group], preferred_element_type=jnp.float32).astype(jnp.bfloat16)
        result = result + partial_sum.astype(jnp.float32)
    return result.astype(jnp.bfloat16)

def run_expert(operands):
    arrived, w_gate, w_up, w_down = operands
    gate_act = jnp.dot(arrived, w_gate, preferred_element_type=jnp.float32)
    up_act = jnp.dot(arrived, w_up, preferred_element_type=jnp.float32)
    hidden = (jax.nn.silu(gate_act) * up_act).astype(jnp.bfloat16)
    group = FF // N_TP
    total = jnp.zeros((arrived.shape[0], D), jnp.float32)
    for part_index in range(N_TP):
        partial_sum = jnp.dot(hidden[:, part_index * group:(part_index + 1) * group], w_down[part_index * group:(part_index + 1) * group], preferred_element_type=jnp.float32).astype(jnp.bfloat16)
        total = total + partial_sum.astype(jnp.float32)
    return total.astype(jnp.bfloat16)

def expert_half(moe_input, moe_gain, gate_weight, up_weight, down_weight, expert_ids, route_weight):
    values = moe_input.astype(jnp.float32)
    normed = (values * lax.rsqrt(lax.optimization_barrier(jnp.mean(values * values, axis=1, keepdims=True)) + eps_rms) * moe_gain).astype(jnp.bfloat16)
    normed_blocks = normed.reshape(N_EP, TOKB_DEV, D)
    id_blocks = expert_ids.reshape(N_EP, TOKB_DEV, TOP)
    slot_index = jax.vmap(lambda ids: slot_numbers(ids, EXPERTS, CAP))(id_blocks)
    sent = jax.vmap(lambda block, slots: fill_slots(block, slots, EXPERTS, CAP, TOP))(normed_blocks, slot_index)
    by_expert = jnp.swapaxes(sent, 0, 1).reshape(EXPERTS, N_EP * CAP, D)
    answers = lax.map(run_expert, (by_expert, gate_weight, up_weight, down_weight))
    answers = jnp.swapaxes(answers.reshape(EXPERTS, N_EP, CAP, D), 0, 1).reshape(N_EP, EXPERTS * CAP, D)

    def combine(block_answers, slots, weights):
        picked = jnp.take(block_answers, slots, axis=0).astype(jnp.float32).reshape(TOKB_DEV, TOP, D)
        return lax.optimization_barrier(jnp.sum(picked * weights[:, :, None], axis=1))
    mixed = jax.vmap(combine)(answers, slot_index, route_weight.reshape(N_EP, TOKB_DEV, TOP))
    return mixed.reshape(N_EP * TOKB_DEV, D).astype(jnp.bfloat16)

def reference(glu_value, glu_gate, conv_kernel, ln_gain, out_weight, moe_input, moe_gain, gate_weight, up_weight, down_weight, expert_ids, route_weight):
    mixer_out = mixer_half(glu_value, glu_gate, conv_kernel, ln_gain, out_weight)
    expert_out = expert_half(moe_input, moe_gain, gate_weight, up_weight, down_weight, expert_ids, route_weight)
    return (mixer_out, expert_out)
```

```python
import functools

import jax
import jax.numpy as jnp
from jax import lax
from jax.experimental import pallas as pl
from jax.experimental.pallas import tpu as pltpu
from jax.sharding import PartitionSpec as P

eps_rms = 1e-06
eps_norm = 1e-05
MESH = pl.DeviceIdType.MESH
F32 = jnp.float32
BF16 = jnp.bfloat16

A2A_S, A2A_R, AGR_S, AGR_R, AGL_S, AGL_R, FWR_S, FWR_R, FWL_S, FWL_R = range(10)
S1R_S, S1R_R, S1L_S, S1L_R, S2R_S, S2R_R, S2L_S, S2L_R, RET_S, RET_R = range(10, 20)


def layout_of(ep_count):
    if ep_count == 64:
        return 8, (0, 7, 1, 4, 3, 5, 2, 6), 2
    return 2, tuple(range(ep_count // 2)), 1


def from_behind(value, axis, by):
    count = lax.axis_size(axis)
    pairs = [(i, i + by) for i in range(count) if 0 <= i + by < count]
    return lax.ppermute(value, axis, pairs)


def moe_kernel(
    cfg,
    moe_in,
    gain,
    ids,
    ids_t,
    route,
    w_gate_hbm,
    w_up_hbm,
    w_down_hbm,
    out,
    wg,
    wu,
    wd,
    normed,
    send_full,
    send_part,
    xin,
    hid,
    part,
    s1r,
    s1l,
    s2r,
    s2l,
    ans,
    ret,
    w_sem,
    sems,
):
    nz, nyc, order, per_chunk, cap = cfg
    ep = lax.axis_index("ep")
    x = lax.axis_index("tp")
    z = ep // nyc
    yc = ep % nyc
    xp, xm, xo = (x + 1) % 4, (x + 3) % 4, (x + 2) % 4
    n_ep = nz * nyc
    n_chunks = nz // per_chunk
    rows = per_chunk * nyc * cap
    half = rows // 2
    group = nyc * cap
    tokens, width = moe_in.shape
    quarter = width // 4

    barrier = pltpu.get_barrier_semaphore()

    def greet(j, c):
        pl.semaphore_signal(
            barrier, inc=1, device_id=((ep + j) % n_ep, x), device_id_type=MESH
        )
        return c

    lax.fori_loop(1, n_ep, greet, 0)
    for other in (xp, xm):
        pl.semaphore_signal(barrier, inc=1, device_id=(ep, other), device_id_type=MESH)

    loads = [
        pltpu.make_async_copy(w_gate_hbm.at[0], wg, w_sem.at[0]),
        pltpu.make_async_copy(w_up_hbm.at[0], wu, w_sem.at[1]),
        pltpu.make_async_copy(w_down_hbm.at[0], wd, w_sem.at[2]),
    ]
    for load in loads:
        load.start()

    def rdma(src, dst, row_s, row_r, k, to_ep, to_x):
        return pltpu.make_async_remote_copy(
            src_ref=src,
            dst_ref=dst,
            send_sem=sems.at[row_s, k],
            recv_sem=sems.at[row_r, k],
            device_id=(to_ep, to_x),
            device_id_type=MESH,
        )

    block = min(32, tokens)

    def norm_rows(i, c):
        at = pl.ds(pl.multiple_of(i * block, block), block)
        v = moe_in[at, :].astype(F32)
        scale = lax.rsqrt(jnp.sum(v * v, axis=1, keepdims=True) / width + eps_rms)
        y = (v * scale * gain[...]).astype(BF16)
        for q in range(4):
            normed[q, at, :] = y[:, q * quarter : (q + 1) * quarter]
        return c

    lax.fori_loop(0, tokens // block, norm_rows, 0)

    def place(e):
        dz = (e // nyc - z + nz) % nz
        pos = jnp.zeros_like(e)
        for p, d in enumerate(order):
            pos = jnp.where(dz == d, p, pos)
        return ((pos * nyc + e % nyc) * cap).astype(F32)

    ti = lax.broadcasted_iota(jnp.int32, (tokens, tokens), 0)
    tj = lax.broadcasted_iota(jnp.int32, (tokens, tokens), 1)
    er = lax.broadcasted_iota(jnp.int32, (64, tokens), 0)
    e0r, e1r = ids_t[0:1, :], ids_t[1:2, :]
    m0r, m1r = er == e0r, er == e1r
    mbr = jnp.where(m0r | m1r, 1.0, 0.0).astype(BF16)
    before = jnp.where(ti < tj, 1.0, 0.0).astype(BF16)
    earlier_r = jnp.dot(mbr, before, preferred_element_type=F32)
    slot0r = place(e0r) + jnp.sum(jnp.where(m0r, earlier_r, 0.0), axis=0, keepdims=True)
    slot1r = place(e1r) + jnp.sum(jnp.where(m1r, earlier_r, 0.0), axis=0, keepdims=True)

    def pick_rows(start, count):
        at = (lax.broadcasted_iota(jnp.int32, (count, tokens), 0) + start).astype(F32)
        return jnp.where((at == slot0r) | (at == slot1r), 1.0, 0.0).astype(BF16)

    for p in range(per_chunk):
        pick = pick_rows(p * group, group)
        for q in range(4):
            send_full[q, p * group : (p + 1) * group, :] = jnp.dot(
                pick, normed[q], preferred_element_type=F32
            ).astype(BF16)

    def fill_part(p, c):
        pick = pick_rows((p + per_chunk) * group, group)
        at = pl.ds(pl.multiple_of(p * group, group), group)
        send_part[at, :] = jnp.dot(pick, normed[x], preferred_element_type=F32).astype(BF16)
        return c

    lax.fori_loop(0, nz - per_chunk, fill_part, 0)

    pl.semaphore_wait(barrier, n_ep - 1 + 2)

    for p in range(nz):
        dz = order[p]
        k = p // per_chunk
        to_z = (z + dz) % nz

        def send(j, c, p=p, dz=dz, k=k, to_z=to_z):
            other = (yc + j) % nyc
            there = pl.ds(pl.multiple_of((p * nyc + yc) * cap, cap), cap)
            if k == 0:
                here = pl.ds(pl.multiple_of((p * nyc + other) * cap, cap), cap)
                copy = rdma(
                    send_full.at[:, here, :],
                    xin.at[:, there, :],
                    A2A_S, A2A_R, k, to_z * nyc + other, x,
                )
            else:
                here = pl.ds(
                    pl.multiple_of(((p - per_chunk) * nyc + other) * cap, cap), cap
                )
                copy = rdma(
                    send_part.at[here, :],
                    xin.at[x, there, :],
                    A2A_S, A2A_R, k, to_z * nyc + other, x,
                )
            copy.start()
            return c

        lax.fori_loop(1 if dz == 0 else 0, nyc, send, 0)

    mine = pl.ds(pl.multiple_of(yc * cap, cap), cap)
    for q in range(4):
        xin[q, mine, :] = send_full[q, mine, :]

    ec = lax.broadcasted_iota(jnp.int32, (tokens, 128), 1)
    e0c, e1c = ids[:, 0:1], ids[:, 1:2]
    m0c, m1c = ec == e0c, ec == e1c
    mbc = jnp.where(m0c | m1c, 1.0, 0.0).astype(BF16)
    after = jnp.where(tj < ti, 1.0, 0.0).astype(BF16)
    earlier_c = jnp.dot(after, mbc, preferred_element_type=F32)
    slot0c = place(e0c) + jnp.sum(jnp.where(m0c, earlier_c, 0.0), axis=1, keepdims=True)
    slot1c = place(e1c) + jnp.sum(jnp.where(m1c, earlier_c, 0.0), axis=1, keepdims=True)

    for load in loads:
        load.wait()

    def at_chunk(k):
        return pl.ds(k * rows, rows)

    def wait_in(k):
        if k == 0:
            region = xin.at[:, pl.ds(0, rows - cap), :]
        else:
            region = xin.at[x, at_chunk(k), :]
        rdma(region, region, A2A_S, A2A_R, k, ep, xp).wait_recv()

    def gather_start(k):
        region = xin.at[x, at_chunk(k), :]
        rdma(region, region, AGR_S, AGR_R, k, ep, xp).start()
        rdma(region, region, AGL_S, AGL_R, k, ep, xm).start()

    def gather_forward(k):
        left = xin.at[xm, at_chunk(k), :]
        rdma(left, left, AGR_S, AGR_R, k, ep, xp).wait_recv()
        top = xin.at[xm, pl.ds(k * rows, half), :]
        rdma(top, top, FWR_S, FWR_R, k, ep, xp).start()
        right = xin.at[xp, at_chunk(k), :]
        rdma(right, right, AGL_S, AGL_R, k, ep, xm).wait_recv()
        low = xin.at[xp, pl.ds(k * rows + half, half), :]
        rdma(low, low, FWL_S, FWL_R, k, ep, xm).start()

    def gather_done(k):
        top = xin.at[xo, pl.ds(k * rows, half), :]
        low = xin.at[xo, pl.ds(k * rows + half, half), :]
        rdma(top, top, FWR_S, FWR_R, k, ep, xp).wait_recv()
        rdma(low, low, FWL_S, FWL_R, k, ep, xm).wait_recv()

    hidden_dev = wg.shape[1]
    nb = min(256, hidden_dev)

    def compute(k):
        def up(n, c):
            cols = pl.ds(pl.multiple_of(n * nb, nb), nb)
            g = jnp.zeros((rows, nb), F32)
            u = jnp.zeros((rows, nb), F32)
            for q in range(4):
                xq = xin[q, at_chunk(k), :]
                ws = pl.ds(q * quarter, quarter)
                g = g + jnp.dot(xq, wg[ws, cols], preferred_element_type=F32)
                u = u + jnp.dot(xq, wu[ws, cols], preferred_element_type=F32)
            hid[:, cols] = (g / (1.0 + jnp.exp(-g)) * u).astype(BF16)
            return c

        lax.fori_loop(0, hidden_dev // nb, up, 0)

        def down(d):
            cols = pl.ds(pl.multiple_of(d * quarter, quarter), quarter)
            part[k, d] = jnp.dot(
                hid[...], wd[:, cols], preferred_element_type=F32
            ).astype(BF16)

        down(xo)
        down(xp)
        rdma(
            part.at[k, xo, pl.ds(0, half), :], s1r.at[k], S1R_S, S1R_R, k, ep, xp
        ).start()
        rdma(
            part.at[k, xo, pl.ds(half, half), :], s1l.at[k], S1L_S, S1L_R, k, ep, xm
        ).start()
        down(xm)
        down(x)

    def scatter_add(k):
        rdma(s1r.at[k], s1r.at[k], S1R_S, S1R_R, k, ep, xp).wait_recv()
        top = pl.ds(0, half)
        part[k, xp, top, :] = (
            part[k, xp, top, :].astype(F32) + s1r[k].astype(F32)
        ).astype(BF16)
        rdma(s1l.at[k], s1l.at[k], S1L_S, S1L_R, k, ep, xm).wait_recv()
        low = pl.ds(half, half)
        part[k, xm, low, :] = (
            part[k, xm, low, :].astype(F32) + s1l[k].astype(F32)
        ).astype(BF16)
        rdma(part.at[k, xp], s2r.at[k], S2R_S, S2R_R, k, ep, xp).start()
        rdma(part.at[k, xm], s2l.at[k], S2L_S, S2L_R, k, ep, xm).start()

    def give_back(k):
        rdma(s2r.at[k], s2r.at[k], S2R_S, S2R_R, k, ep, xp).wait_recv()
        rdma(s2l.at[k], s2l.at[k], S2L_S, S2L_R, k, ep, xm).wait_recv()
        total = part[k, x].astype(F32) + s2r[k].astype(F32) + s2l[k].astype(F32)
        ans[at_chunk(k), :] = total.astype(BF16)
        if k == 0:
            ret[mine, :] = ans[mine, :]
        for p in range(k * per_chunk, (k + 1) * per_chunk):
            dz = order[p]
            to_z = (z - dz + nz) % nz

            def send(j, c, p=p, to_z=to_z):
                other = (yc + j) % nyc
                here = pl.ds(pl.multiple_of((p * nyc + other) * cap, cap), cap)
                there = pl.ds(pl.multiple_of((p * nyc + yc) * cap, cap), cap)
                rdma(
                    ans.at[here, :], ret.at[there, :], RET_S, RET_R, k,
                    to_z * nyc + other, x,
                ).start()
                return c

            lax.fori_loop(1 if dz == 0 else 0, nyc, send, 0)

    wait_in(0)
    compute(0)
    if n_chunks > 1:
        wait_in(1)
        gather_start(1)
    for k in range(n_chunks):
        scatter_add(k)
        if k + 1 < n_chunks:
            gather_forward(k + 1)
        if k + 2 < n_chunks:
            wait_in(k + 2)
            gather_start(k + 2)
        if k + 1 < n_chunks:
            gather_done(k + 1)
            compute(k + 1)
        give_back(k)

    total = jnp.zeros((tokens, quarter), F32)
    w0, w1 = route[:, 0:1], route[:, 1:2]
    for k in range(n_chunks):
        count = rows - cap if k == 0 else rows
        region = ret.at[pl.ds(k * rows, count), :]
        rdma(region, region, RET_S, RET_R, k, ep, xp).wait_recv()
        at = (lax.broadcasted_iota(jnp.int32, (tokens, rows), 1) + k * rows).astype(F32)
        w = jnp.where(at == slot0c, w0, 0.0) + jnp.where(at == slot1c, w1, 0.0)
        high = w.astype(BF16)
        low = (w - high.astype(F32)).astype(BF16)
        got = ret[at_chunk(k), :]
        total = total + jnp.dot(high, got, preferred_element_type=F32)
        total = total + jnp.dot(low, got, preferred_element_type=F32)
    out[...] = total.astype(BF16)

    for k in range(n_chunks):
        if k == 0:
            region = send_full.at[:, pl.ds(0, rows - cap), :]
            back = ans.at[pl.ds(0, rows - cap), :]
        else:
            region = send_part.at[pl.ds((k - 1) * rows, rows), :]
            back = ans.at[at_chunk(k), :]
            whole = xin.at[x, at_chunk(k), :]
            part_half = xin.at[xm, pl.ds(k * rows, half), :]
            rdma(whole, whole, AGR_S, AGR_R, k, ep, xp).wait_send()
            rdma(whole, whole, AGL_S, AGL_R, k, ep, xm).wait_send()
            rdma(part_half, part_half, FWR_S, FWR_R, k, ep, xp).wait_send()
            rdma(part_half, part_half, FWL_S, FWL_R, k, ep, xm).wait_send()
        rdma(region, region, A2A_S, A2A_R, k, ep, xp).wait_send()
        rdma(s1r.at[k], s1r.at[k], S1R_S, S1R_R, k, ep, xp).wait_send()
        rdma(s1l.at[k], s1l.at[k], S1L_S, S1L_R, k, ep, xm).wait_send()
        rdma(s2r.at[k], s2r.at[k], S2R_S, S2R_R, k, ep, xp).wait_send()
        rdma(s2l.at[k], s2l.at[k], S2L_S, S2L_R, k, ep, xm).wait_send()
        rdma(back, back, RET_S, RET_R, k, ep, xp).wait_send()


def run_experts(moe_input, moe_gain, gate_weight, up_weight, down_weight, expert_ids, route_weight):
    tokens, width = moe_input.shape
    ep_count = lax.axis_size("ep")
    nyc, order, per_chunk = layout_of(ep_count)
    nz = ep_count // nyc
    cap = 16
    hidden_dev = gate_weight.shape[2]
    quarter = width // 4
    n_chunks = nz // per_chunk
    rows = per_chunk * nyc * cap
    slots = ep_count * cap
    vmem = pl.BlockSpec(memory_space=pltpu.VMEM)
    hbm = pl.BlockSpec(memory_space=pl.ANY)
    cfg = (nz, nyc, order, per_chunk, cap)
    return pl.pallas_call(
        functools.partial(moe_kernel, cfg),
        out_shape=jax.ShapeDtypeStruct((tokens, quarter), BF16),
        in_specs=[vmem] * 5 + [hbm] * 3,
        out_specs=vmem,
        scratch_shapes=[
            pltpu.VMEM((width, hidden_dev), BF16),
            pltpu.VMEM((width, hidden_dev), BF16),
            pltpu.VMEM((hidden_dev, width), BF16),
            pltpu.VMEM((4, tokens, quarter), BF16),
            pltpu.VMEM((4, rows, quarter), BF16),
            pltpu.VMEM((max(slots - rows, rows), quarter), BF16),
            pltpu.VMEM((4, slots, quarter), BF16),
            pltpu.VMEM((rows, hidden_dev), BF16),
            pltpu.VMEM((n_chunks, 4, rows, quarter), BF16),
            pltpu.VMEM((n_chunks, rows // 2, quarter), BF16),
            pltpu.VMEM((n_chunks, rows // 2, quarter), BF16),
            pltpu.VMEM((n_chunks, rows, quarter), BF16),
            pltpu.VMEM((n_chunks, rows, quarter), BF16),
            pltpu.VMEM((slots, quarter), BF16),
            pltpu.VMEM((slots, quarter), BF16),
            pltpu.SemaphoreType.DMA((3,)),
            pltpu.SemaphoreType.DMA((20, n_chunks)),
        ],
        compiler_params=pltpu.CompilerParams(
            collective_id=0, has_side_effects=True, vmem_limit_bytes=60 * 1024 * 1024
        ),
        cost_estimate=pl.CostEstimate(
            flops=10_000_000_000, bytes_accessed=12_000_000, transcendentals=0
        ),
        name="experts",
    )(
        moe_input,
        moe_gain[None, :],
        expert_ids,
        expert_ids.T,
        route_weight,
        gate_weight,
        up_weight,
        down_weight,
    )


def on_device(
    glu_value,
    glu_gate,
    conv_kernel,
    ln_gain,
    out_weight,
    moe_input,
    moe_gain,
    gate_weight,
    up_weight,
    down_weight,
    expert_ids,
    route_weight,
):
    length, channels_dev = glu_value.shape
    reach = conv_kernel.shape[0]
    tp_count = lax.axis_size("tp")
    gated = (glu_value.astype(F32) * jax.nn.sigmoid(glu_gate.astype(F32))).astype(BF16)
    earlier_rows = from_behind(gated[length - (reach - 1) :], "ep", 1)
    padded = jnp.concatenate([earlier_rows, gated], axis=0).astype(F32)
    convolved = jnp.zeros((length, channels_dev), F32)
    for tap_index in range(reach):
        begin = reach - 1 - tap_index
        convolved = convolved + conv_kernel[tap_index] * padded[begin : begin + length]
    total, squares = lax.psum(
        (jnp.sum(convolved, axis=1), jnp.sum(convolved * convolved, axis=1)), "tp"
    )
    channels = channels_dev * tp_count
    mean = total / channels
    variance = squares / channels - mean * mean
    scaled = (convolved - mean[:, None]) * lax.rsqrt(variance + eps_norm)[:, None] * ln_gain
    activated = jax.nn.silu(scaled).astype(BF16)
    partial_sum = jnp.dot(activated, out_weight, preferred_element_type=F32).astype(BF16)
    partial_sum, moe_input = lax.optimization_barrier((partial_sum, moe_input))
    mixer_out = lax.psum_scatter(partial_sum, "tp", scatter_dimension=0, tiled=True)
    expert_out = run_experts(
        moe_input, moe_gain, gate_weight, up_weight, down_weight, expert_ids, route_weight
    )
    return (mixer_out, expert_out)


def solution(mesh):
    in_specs = (
        P("ep", "tp"),
        P("ep", "tp"),
        P(None, "tp"),
        P("tp"),
        P("tp", None),
        P("ep", None),
        P(),
        P("ep", None, "tp"),
        P("ep", None, "tp"),
        P("ep", "tp", None),
        P("ep", None),
        P("ep", None),
    )
    out_specs = (P(("ep", "tp"), None), P("ep", "tp"))
    return jax.shard_map(
        on_device, mesh=mesh, in_specs=in_specs, out_specs=out_specs, check_vma=False
    )
```

```python
import functools

import jax
import jax.numpy as jnp
from jax import lax
from jax.experimental import pallas as pl
from jax.experimental.pallas import tpu as pltpu
from jax.sharding import PartitionSpec as P

eps_rms = 1e-06
eps_norm = 1e-05
MESH = pl.DeviceIdType.MESH
F32 = jnp.float32
BF16 = jnp.bfloat16

A2A_S, A2A_R, AGR_S, AGR_R, AGL_S, AGL_R, FWR_S, FWR_R, FWL_S, FWL_R = range(10)
S1R_S, S1R_R, S1L_S, S1L_R, S2R_S, S2R_R, S2L_S, S2L_R, RET_S, RET_R = range(10, 20)
A2P_S, A2P_R = 20, 21
HALO, STAT_P, STAT_M, STAT_O, ACT_P, ACT_M, ACT_O, WR, WL, WFR, WFL, WC_P, WC_M, WC_O = range(14)


def layout_of(ep_count):
    if ep_count == 64:
        return 8, (5, 3, 6, 4, 7, 2, 0, 1), (0, 0, 0, 0, 1, 1, 1, 1), 2
    return 2, (2, 3, 1, 0), (0, 0, 1, 1), 1


def block_kernel(
    cfg,
    gain,
    ids_t,
    route_t,
    taps,
    ln_gain,
    moe_hbm,
    value_hbm,
    gate_hbm,
    w_out_hbm,
    w_gate_hbm,
    w_up_hbm,
    w_down_hbm,
    mixed,
    out,
    moe_in,
    value,
    gate,
    w_out,
    wg,
    wu,
    wd,
    normed,
    send_full,
    send_part,
    xin,
    hid,
    part,
    s1r,
    s1l,
    s2r,
    s2l,
    ans,
    ret,
    tail,
    halo,
    gated,
    conv,
    stat,
    stat_in,
    act,
    act_in,
    total,
    w_sem,
    sems,
    msend,
    mrecv,
):
    nz, nyc, order, whole, per_chunk, cap = cfg
    ep = lax.axis_index("ep")
    x = lax.axis_index("tp")
    z = ep // nyc
    yc = ep % nyc
    xp, xm, xo = (x + 1) % 4, (x + 3) % 4, (x + 2) % 4
    n_ep = nz * nyc
    n_chunks = nz // per_chunk
    rows = per_chunk * nyc * cap
    half = rows // 2
    group = nyc * cap
    tokens, width = moe_in.shape
    quarter = width // 4
    whole_at = {p: sum(whole[:p]) for p in range(nz) if whole[p]}
    part_at = {p: p - sum(whole[:p]) for p in range(nz) if not whole[p]}
    own = order.index(0)

    barrier = pltpu.get_barrier_semaphore()

    def greet(j, c):
        pl.semaphore_signal(
            barrier, inc=1, device_id=((ep + j) % n_ep, x), device_id_type=MESH
        )
        return c

    lax.fori_loop(1, n_ep, greet, 0)
    for other in (xp, xm, xo):
        pl.semaphore_signal(barrier, inc=1, device_id=(ep, other), device_id_type=MESH)

    loads = [
        pltpu.make_async_copy(src, dst, w_sem.at[i])
        for i, (src, dst) in enumerate(
            (
                (moe_hbm, moe_in),
                (value_hbm, value),
                (gate_hbm, gate),
                (w_out_hbm, w_out.at[x]),
                (w_gate_hbm.at[0], wg),
                (w_up_hbm.at[0], wu),
                (w_down_hbm.at[0], wd),
            )
        )
    ]
    for load in loads:
        load.start()

    def rdma(src, dst, row_s, row_r, k, to_ep, to_x):
        return pltpu.make_async_remote_copy(
            src_ref=src,
            dst_ref=dst,
            send_sem=sems.at[row_s, k],
            recv_sem=sems.at[row_r, k],
            device_id=(to_ep, to_x),
            device_id_type=MESH,
        )

    block = min(32, tokens)

    def norm_rows(i, c):
        at = pl.ds(pl.multiple_of(i * block, block), block)
        v = moe_in[at, :].astype(F32)
        scale = lax.rsqrt(jnp.sum(v * v, axis=1, keepdims=True) / width + eps_rms)
        y = (v * scale * gain[...]).astype(BF16)
        for q in range(4):
            normed[q, at, :] = y[:, q * quarter : (q + 1) * quarter]
        return c

    def place(e):
        dz = (e // nyc - z + nz) % nz
        pos = jnp.zeros_like(e)
        for p, d in enumerate(order):
            pos = jnp.where(dz == d, p, pos)
        return ((pos * nyc + e % nyc) * cap).astype(F32)

    with jax.named_scope("slots"):
        ti = lax.broadcasted_iota(jnp.int32, (tokens, tokens), 0)
        tj = lax.broadcasted_iota(jnp.int32, (tokens, tokens), 1)
        er = lax.broadcasted_iota(jnp.int32, (64, tokens), 0)
        e0r, e1r = ids_t[0:1, :], ids_t[1:2, :]
        hit0, hit1 = er == e0r, er == e1r
        mbr = jnp.where(hit0 | hit1, 1.0, 0.0).astype(BF16)
        before = jnp.where(ti < tj, 1.0, 0.0).astype(BF16)
        earlier_r = jnp.dot(mbr, before, preferred_element_type=F32)
        slot0r = place(e0r) + jnp.sum(jnp.where(hit0, earlier_r, 0.0), axis=0, keepdims=True)
        slot1r = place(e1r) + jnp.sum(jnp.where(hit1, earlier_r, 0.0), axis=0, keepdims=True)

    def pick_rows(start, count):
        at = (lax.broadcasted_iota(jnp.int32, (count, tokens), 0) + start).astype(F32)
        return jnp.where((at == slot0r) | (at == slot1r), 1.0, 0.0).astype(BF16)

    def fill(p):
        pick = pick_rows(p * group, group)
        if whole[p]:
            at = pl.ds(whole_at[p] * group, group)
            for q in range(4):
                send_full[q, at, :] = jnp.dot(
                    pick, normed[q], preferred_element_type=F32
                ).astype(BF16)
        else:
            at = pl.ds(part_at[p] * group, group)
            send_part[at, :] = jnp.dot(pick, normed[x], preferred_element_type=F32).astype(BF16)

    def send_rows(p):
        dz = order[p]
        k = p // per_chunk
        to_z = (z + dz) % nz

        def send(j, c):
            other = (yc + j) % nyc
            there = pl.ds(pl.multiple_of((p * nyc + yc) * cap, cap), cap)
            if whole[p]:
                here = pl.ds(pl.multiple_of((whole_at[p] * nyc + other) * cap, cap), cap)
                copy = rdma(
                    send_full.at[:, here, :],
                    xin.at[:, there, :],
                    A2A_S, A2A_R, k, to_z * nyc + other, x,
                )
            else:
                here = pl.ds(pl.multiple_of((part_at[p] * nyc + other) * cap, cap), cap)
                copy = rdma(
                    send_part.at[here, :],
                    xin.at[x, there, :],
                    A2P_S, A2P_R, k, to_z * nyc + other, x,
                )
            copy.start()
            return c

        lax.fori_loop(1 if dz == 0 else 0, nyc, send, 0)

    def send_chunk(k):
        for p in range(k * per_chunk, (k + 1) * per_chunk):
            fill(p)
        for p in range(k * per_chunk, (k + 1) * per_chunk):
            send_rows(p)

    mine = pl.ds(pl.multiple_of((own * nyc + yc) * cap, cap), cap)

    def keep_own():
        if whole[own]:
            here = pl.ds(pl.multiple_of((whole_at[own] * nyc + yc) * cap, cap), cap)
            for q in range(4):
                xin[q, mine, :] = send_full[q, here, :]
        else:
            here = pl.ds(pl.multiple_of((part_at[own] * nyc + yc) * cap, cap), cap)
            xin[x, mine, :] = send_part[here, :]

    def at_chunk(k):
        return pl.ds(k * rows, rows)

    def parts_of(k):
        n = sum(whole[k * per_chunk : (k + 1) * per_chunk]) * group
        return k * rows, n, k * rows + n, rows - n

    def less_own(k, is_whole):
        return cap if own // per_chunk == k and bool(whole[own]) == is_whole else 0

    def wait_in(k):
        w0, wn, g0, gn = parts_of(k)
        if wn:
            region = xin.at[:, pl.ds(w0, wn - less_own(k, True)), :]
            rdma(region, region, A2A_S, A2A_R, k, ep, xp).wait_recv()
        if gn:
            region = xin.at[x, pl.ds(g0, gn - less_own(k, False)), :]
            rdma(region, region, A2P_S, A2P_R, k, ep, xp).wait_recv()

    def gather_start(k):
        _, _, g0, gn = parts_of(k)
        if gn:
            region = xin.at[x, pl.ds(g0, gn), :]
            rdma(region, region, AGR_S, AGR_R, k, ep, xp).start()
            rdma(region, region, AGL_S, AGL_R, k, ep, xm).start()

    def gather_forward(k):
        _, _, g0, gn = parts_of(k)
        if gn:
            left = xin.at[xm, pl.ds(g0, gn), :]
            rdma(left, left, AGR_S, AGR_R, k, ep, xp).wait_recv()
            top = xin.at[xm, pl.ds(g0, gn // 2), :]
            rdma(top, top, FWR_S, FWR_R, k, ep, xp).start()
            right = xin.at[xp, pl.ds(g0, gn), :]
            rdma(right, right, AGL_S, AGL_R, k, ep, xm).wait_recv()
            low = xin.at[xp, pl.ds(g0 + gn // 2, gn // 2), :]
            rdma(low, low, FWL_S, FWL_R, k, ep, xm).start()

    def gather_done(k):
        _, _, g0, gn = parts_of(k)
        if gn:
            top = xin.at[xo, pl.ds(g0, gn // 2), :]
            low = xin.at[xo, pl.ds(g0 + gn // 2, gn // 2), :]
            rdma(top, top, FWR_S, FWR_R, k, ep, xp).wait_recv()
            rdma(low, low, FWL_S, FWL_R, k, ep, xm).wait_recv()

    hidden_dev = wg.shape[1]
    nb = min(256, hidden_dev)

    def compute(k):
        def up(n, c):
            cols = pl.ds(pl.multiple_of(n * nb, nb), nb)
            g = jnp.zeros((rows, nb), F32)
            u = jnp.zeros((rows, nb), F32)
            for q in range(4):
                xq = xin[q, at_chunk(k), :]
                ws = pl.ds(q * quarter, quarter)
                g = g + jnp.dot(xq, wg[ws, cols], preferred_element_type=F32)
                u = u + jnp.dot(xq, wu[ws, cols], preferred_element_type=F32)
            hid[:, cols] = (g / (1.0 + jnp.exp(-g)) * u).astype(BF16)
            return c

        lax.fori_loop(0, hidden_dev // nb, up, 0)

        def down(d):
            cols = pl.ds(pl.multiple_of(d * quarter, quarter), quarter)
            part[k, d] = jnp.dot(
                hid[...], wd[:, cols], preferred_element_type=F32
            ).astype(BF16)

        down(xo)
        down(xp)
        rdma(
            part.at[k, xo, pl.ds(0, half), :], s1r.at[k], S1R_S, S1R_R, k, ep, xp
        ).start()
        rdma(
            part.at[k, xo, pl.ds(half, half), :], s1l.at[k], S1L_S, S1L_R, k, ep, xm
        ).start()
        down(xm)
        down(x)

    def scatter_add(k):
        rdma(s1r.at[k], s1r.at[k], S1R_S, S1R_R, k, ep, xp).wait_recv()
        top = pl.ds(0, half)
        part[k, xp, top, :] = (
            part[k, xp, top, :].astype(F32) + s1r[k].astype(F32)
        ).astype(BF16)
        rdma(s1l.at[k], s1l.at[k], S1L_S, S1L_R, k, ep, xm).wait_recv()
        low = pl.ds(half, half)
        part[k, xm, low, :] = (
            part[k, xm, low, :].astype(F32) + s1l[k].astype(F32)
        ).astype(BF16)
        rdma(part.at[k, xp], s2r.at[k], S2R_S, S2R_R, k, ep, xp).start()
        rdma(part.at[k, xm], s2l.at[k], S2L_S, S2L_R, k, ep, xm).start()

    def give_back(k):
        rdma(s2r.at[k], s2r.at[k], S2R_S, S2R_R, k, ep, xp).wait_recv()
        rdma(s2l.at[k], s2l.at[k], S2L_S, S2L_R, k, ep, xm).wait_recv()
        sums = part[k, x].astype(F32) + s2r[k].astype(F32) + s2l[k].astype(F32)
        ans[at_chunk(k), :] = sums.astype(BF16)
        if k == own // per_chunk:
            ret[mine, :] = ans[mine, :]
        for p in range(k * per_chunk, (k + 1) * per_chunk):
            dz = order[p]
            to_z = (z - dz + nz) % nz

            def send(j, c, p=p, to_z=to_z):
                other = (yc + j) % nyc
                here = pl.ds(pl.multiple_of((p * nyc + other) * cap, cap), cap)
                there = pl.ds(pl.multiple_of((p * nyc + yc) * cap, cap), cap)
                rdma(
                    ans.at[here, :], ret.at[there, :], RET_S, RET_R, k,
                    to_z * nyc + other, x,
                ).start()
                return c

            lax.fori_loop(1 if dz == 0 else 0, nyc, send, 0)

    length, channels_dev = value.shape
    lane_groups = channels_dev // 128
    reach = taps.shape[0]
    m_rows = length // 4
    core = ep % 2
    partner = ep + 1 - 2 * core
    w_half = channels_dev // 2
    w_mine = pl.ds(pl.multiple_of(core * w_half, w_half), w_half)
    w_theirs = pl.ds(pl.multiple_of((1 - core) * w_half, w_half), w_half)
    w_top = pl.ds(pl.multiple_of(core * w_half, w_half // 2), w_half // 2)
    w_low = pl.ds(pl.multiple_of(core * w_half + w_half // 2, w_half // 2), w_half // 2)

    def mcopy(src, dst, row, to_ep, to_x):
        return pltpu.make_async_remote_copy(
            src_ref=src,
            dst_ref=dst,
            send_sem=msend.at[row],
            recv_sem=mrecv.at[row],
            device_id=(to_ep, to_x),
            device_id_type=MESH,
        )

    def mixer_gate():
        loads[1].wait()
        loads[2].wait()

        def rows_of(i, c):
            at = pl.ds(pl.multiple_of(i * 32, 32), 32)
            v = value[at, :].astype(F32)
            g = gate[at, :].astype(F32)
            y = (v * (1.0 / (1.0 + jnp.exp(-g)))).astype(BF16)
            wide = y.astype(F32)
            to = pl.ds(pl.multiple_of(i * 32 + 32, 32), 32)
            for h in range(lane_groups):
                gated[h, to, :] = wide[:, h * 128 : (h + 1) * 128]
            tail[...] = y
            return c

        lax.fori_loop(0, length // 32, rows_of, 0)

    def halo_send():
        mcopy(tail, halo, HALO, (ep + 1) % n_ep, x).start()

    def mixer_conv():
        mcopy(tail, halo, HALO, (ep + 1) % n_ep, x).wait_recv()
        before_first = jnp.where(ep == 0, 0.0, halo[...].astype(F32))
        for h in range(lane_groups):
            gated[h, 0:32, :] = before_first[:, h * 128 : (h + 1) * 128]
        cb = 64
        for h in range(lane_groups):
            lanes = slice(h * 128, (h + 1) * 128)

            def rows_of(i, c, h=h, lanes=lanes):
                base = pl.multiple_of(i * cb, cb)
                window = gated.at[h, pl.ds(base, cb + 32), :]
                acc = jnp.zeros((cb, 128), F32)
                for j in range(reach):
                    acc = acc + taps[j : j + 1, lanes] * window[32 - j : 32 - j + cb, :]
                conv[pl.ds(base, cb), lanes] = acc
                return c

            lax.fori_loop(0, length // cb, rows_of, 0)

        sb = 128
        lane = lax.broadcasted_iota(jnp.int32, (sb, 128), 1)
        for i in range(length // sb):
            c = conv[i * sb : (i + 1) * sb, :]
            total = jnp.sum(c, axis=1, keepdims=True)
            squares = jnp.sum(c * c, axis=1, keepdims=True)
            both = jnp.where(lane == 0, total, jnp.where(lane == 1, squares, 0.0))
            stat[:, i * sb : (i + 1) * sb] = both.T[0:8, :]
        for n, (row, to_x) in enumerate(((STAT_P, xp), (STAT_M, xm), (STAT_O, xo))):
            mcopy(stat, stat_in.at[n], row, ep, to_x).start()

    def mixer_out():
        for n, row in enumerate((STAT_P, STAT_M, STAT_O)):
            mcopy(stat, stat_in.at[n], row, ep, xp).wait_recv()
        sums = stat[...] + stat_in[0] + stat_in[1] + stat_in[2]
        channels = channels_dev * 4
        sb = 128
        for i in range(length // sb):
            at = slice(i * sb, (i + 1) * sb)
            mean = sums[0:1, at] / channels
            variance = sums[1:2, at] / channels - mean * mean
            scale = lax.rsqrt(variance + eps_norm)
            r = lax.broadcasted_iota(jnp.int32, (128, sb), 0)
            cols = jnp.where(r == 0, mean, jnp.where(r == 1, scale, 0.0)).T
            v = (conv[at, :] - cols[:, 0:1]) * cols[:, 1:2] * ln_gain[...]
            act[at, :] = (v / (1.0 + jnp.exp(-v))).astype(BF16)
        for row, to_x in ((ACT_P, xp), (ACT_M, xm), (ACT_O, xo)):
            at = pl.ds(pl.multiple_of(to_x * m_rows, m_rows), m_rows)
            mcopy(act.at[at, :], act_in.at[x], row, ep, to_x).start()
        act_in[x] = act[pl.ds(pl.multiple_of(x * m_rows, m_rows), m_rows), :]

    def w_start():
        loads[3].wait()
        mcopy(w_out.at[x, w_mine, :], w_out.at[x, w_mine, :], WR, ep, xp).start()
        mcopy(w_out.at[x, w_mine, :], w_out.at[x, w_mine, :], WL, ep, xm).start()

    def w_forward():
        left = w_out.at[xm, w_mine, :]
        mcopy(left, left, WR, ep, xp).wait_recv()
        top = w_out.at[xm, w_top, :]
        mcopy(top, top, WFR, ep, xp).start()
        mcopy(left, left, WC_M, partner, x).start()
        right = w_out.at[xp, w_mine, :]
        mcopy(right, right, WL, ep, xm).wait_recv()
        low = w_out.at[xp, w_low, :]
        mcopy(low, low, WFL, ep, xm).start()
        mcopy(right, right, WC_P, partner, x).start()

    def w_share():
        top = w_out.at[xo, w_top, :]
        low = w_out.at[xo, w_low, :]
        mcopy(top, top, WFR, ep, xp).wait_recv()
        mcopy(low, low, WFL, ep, xm).wait_recv()
        opposite = w_out.at[xo, w_mine, :]
        mcopy(opposite, opposite, WC_O, partner, x).start()

    def mixer_project():
        for row, q in ((ACT_P, xm), (ACT_M, xp), (ACT_O, xo)):
            mcopy(act_in.at[q], act_in.at[q], row, ep, xp).wait_recv()
        for row, q in ((WC_M, xm), (WC_P, xp), (WC_O, xo)):
            theirs = w_out.at[q, w_theirs, :]
            mcopy(theirs, theirs, row, partner, x).wait_recv()

        def project(n, c):
            cols = pl.ds(pl.multiple_of(n * 256, 256), 256)
            sums = jnp.zeros((m_rows, 256), F32)
            for q in range(4):
                sums = sums + jnp.dot(act_in[q], w_out[q, :, cols], preferred_element_type=F32)
            mixed[:, cols] = sums.astype(BF16)
            return c

        lax.fori_loop(0, width // 256, project, 0)

    def combine(k):
        region = ret.at[pl.ds(k * rows, rows - less_own(k, bool(whole[own]))), :]
        rdma(region, region, RET_S, RET_R, k, ep, xp).wait_recv()
        slot0c, slot1c = columns[:, 0:1], columns[:, 1:2]
        at = (lax.broadcasted_iota(jnp.int32, (tokens, rows), 1) + k * rows).astype(F32)
        w = jnp.where(at == slot0c, columns[:, 2:3], 0.0)
        w = w + jnp.where(at == slot1c, columns[:, 3:4], 0.0)
        high = w.astype(BF16)
        low = (w - high.astype(F32)).astype(BF16)
        got = ret[at_chunk(k), :]
        sums = jnp.dot(high, got, preferred_element_type=F32)
        sums = sums + jnp.dot(low, got, preferred_element_type=F32)
        total[...] = sums if k == 0 else total[...] + sums

    def run(step, *k):
        with jax.named_scope(step.__name__ + "".join(f"#{i}" for i in k)):
            step(*k)

    run(mixer_gate)
    with jax.named_scope("barrier_wait"):
        pl.semaphore_wait(barrier, n_ep - 1 + 3)
    halo_send()
    run(w_start)
    with jax.named_scope("norm"):
        loads[0].wait()
        lax.fori_loop(0, tokens // block, norm_rows, 0)
    for k in range(n_chunks):
        run(send_chunk, k)
    keep_own()
    turn = lax.broadcasted_iota(jnp.int32, (128, tokens), 0)
    table = jnp.where(turn == 0, slot0r, jnp.where(turn == 1, slot1r, 0.0))
    table = jnp.where(turn == 2, route_t[0:1, :], table)
    table = jnp.where(turn == 3, route_t[1:2, :], table)
    columns = table.T

    def compute_after(k):
        run(wait_in, k)
        run(gather_done, k)
        run(compute, k)

    run(mixer_conv)
    run(wait_in, 0)
    run(gather_start, 0)
    run(mixer_out)
    run(w_forward)
    run(gather_forward, 0)
    for load in loads[4:]:
        load.wait()
    run(gather_done, 0)
    run(compute, 0)
    run(w_share)
    run(wait_in, 1)
    run(gather_start, 1)
    run(scatter_add, 0)
    run(gather_forward, 1)
    run(mixer_project)
    run(give_back, 0)
    run(gather_done, 1)
    run(compute, 1)
    run(wait_in, 2)
    run(gather_start, 2)
    run(gather_forward, 2)
    run(gather_done, 2)
    run(compute, 2)
    run(scatter_add, 1)
    run(wait_in, 3)
    run(compute, 3)
    run(scatter_add, 2)
    run(give_back, 1)
    run(combine, 0)
    run(scatter_add, 3)
    run(give_back, 2)
    run(combine, 1)
    run(give_back, 3)
    run(combine, 2)
    run(combine, 3)
    out[...] = total[...].astype(BF16)

    for k in range(n_chunks):
        w0, wn, g0, gn = parts_of(k)
        if wn:
            region = send_full.at[:, pl.ds(0, wn - less_own(k, True)), :]
            rdma(region, region, A2A_S, A2A_R, k, ep, xp).wait_send()
        if gn:
            region = send_part.at[pl.ds(0, gn - less_own(k, False)), :]
            rdma(region, region, A2P_S, A2P_R, k, ep, xp).wait_send()
            region = xin.at[x, pl.ds(g0, gn), :]
            rdma(region, region, AGR_S, AGR_R, k, ep, xp).wait_send()
            rdma(region, region, AGL_S, AGL_R, k, ep, xm).wait_send()
            region = xin.at[x, pl.ds(g0, gn // 2), :]
            rdma(region, region, FWR_S, FWR_R, k, ep, xp).wait_send()
            rdma(region, region, FWL_S, FWL_R, k, ep, xm).wait_send()
        back = ans.at[pl.ds(k * rows, rows - less_own(k, bool(whole[own]))), :]
        rdma(s1r.at[k], s1r.at[k], S1R_S, S1R_R, k, ep, xp).wait_send()
        rdma(s1l.at[k], s1l.at[k], S1L_S, S1L_R, k, ep, xm).wait_send()
        rdma(s2r.at[k], s2r.at[k], S2R_S, S2R_R, k, ep, xp).wait_send()
        rdma(s2l.at[k], s2l.at[k], S2L_S, S2L_R, k, ep, xm).wait_send()
        rdma(back, back, RET_S, RET_R, k, ep, xp).wait_send()
    mcopy(tail, tail, HALO, ep, xp).wait_send()
    for row in (STAT_P, STAT_M, STAT_O):
        mcopy(stat, stat, row, ep, xp).wait_send()
    for row in (ACT_P, ACT_M, ACT_O):
        mcopy(act_in.at[0], act_in.at[0], row, ep, xp).wait_send()
    for row in (WR, WL, WC_P, WC_M, WC_O):
        sent = w_out.at[x, w_mine, :]
        mcopy(sent, sent, row, ep, xp).wait_send()
    for row in (WFR, WFL):
        sent = w_out.at[x, w_top, :]
        mcopy(sent, sent, row, ep, xp).wait_send()


def on_device(
    glu_value,
    glu_gate,
    conv_kernel,
    ln_gain,
    out_weight,
    moe_input,
    moe_gain,
    gate_weight,
    up_weight,
    down_weight,
    expert_ids,
    route_weight,
):
    tokens, width = moe_input.shape
    length, channels_dev = glu_value.shape
    ep_count = lax.axis_size("ep")
    nyc, order, whole, per_chunk = layout_of(ep_count)
    nz = ep_count // nyc
    cap = 16
    hidden_dev = gate_weight.shape[2]
    quarter = width // 4
    n_chunks = nz // per_chunk
    rows = per_chunk * nyc * cap
    slots = ep_count * cap
    vmem = pl.BlockSpec(memory_space=pltpu.VMEM)
    hbm = pl.BlockSpec(memory_space=pl.ANY)
    n_whole = sum(whole) * nyc * cap
    cfg = (nz, nyc, order, whole, per_chunk, cap)
    return pl.pallas_call(
        functools.partial(block_kernel, cfg),
        out_shape=(
            jax.ShapeDtypeStruct((length // 4, width), BF16),
            jax.ShapeDtypeStruct((tokens, quarter), BF16),
        ),
        in_specs=[vmem] * 5 + [hbm] * 7,
        out_specs=(vmem, vmem),
        scratch_shapes=[
            pltpu.VMEM((tokens, width), BF16),
            pltpu.VMEM((length, channels_dev), BF16),
            pltpu.VMEM((length, channels_dev), BF16),
            pltpu.VMEM((4, channels_dev, width), BF16),
            pltpu.VMEM((width, hidden_dev), BF16),
            pltpu.VMEM((width, hidden_dev), BF16),
            pltpu.VMEM((hidden_dev, width), BF16),
            pltpu.VMEM((4, tokens, quarter), BF16),
            pltpu.VMEM((4, max(n_whole, 16), quarter), BF16),
            pltpu.VMEM((max(slots - n_whole, 16), quarter), BF16),
            pltpu.VMEM((4, slots, quarter), BF16),
            pltpu.VMEM((rows, hidden_dev), BF16),
            pltpu.VMEM((n_chunks, 4, rows, quarter), BF16),
            pltpu.VMEM((n_chunks, rows // 2, quarter), BF16),
            pltpu.VMEM((n_chunks, rows // 2, quarter), BF16),
            pltpu.VMEM((n_chunks, rows, quarter), BF16),
            pltpu.VMEM((n_chunks, rows, quarter), BF16),
            pltpu.VMEM((slots, quarter), BF16),
            pltpu.VMEM((slots, quarter), BF16),
            pltpu.VMEM((32, channels_dev), BF16),
            pltpu.VMEM((32, channels_dev), BF16),
            pltpu.VMEM((channels_dev // 128, length + 32, 128), F32),
            pltpu.VMEM((length, channels_dev), F32),
            pltpu.VMEM((8, length), F32),
            pltpu.VMEM((3, 8, length), F32),
            pltpu.VMEM((length, channels_dev), BF16),
            pltpu.VMEM((4, length // 4, channels_dev), BF16),
            pltpu.VMEM((tokens, quarter), F32),
            pltpu.SemaphoreType.DMA((7,)),
            pltpu.SemaphoreType.DMA((22, n_chunks)),
            pltpu.SemaphoreType.DMA((14,)),
            pltpu.SemaphoreType.DMA((14,)),
        ],
        compiler_params=pltpu.CompilerParams(
            collective_id=0, has_side_effects=True, vmem_limit_bytes=60 * 1024 * 1024
        ),
        name="block",
    )(
        moe_gain[None, :],
        expert_ids.T,
        route_weight.T,
        conv_kernel,
        ln_gain[None, :],
        moe_input,
        glu_value,
        glu_gate,
        out_weight,
        gate_weight,
        up_weight,
        down_weight,
    )


def solution(mesh):
    in_specs = (
        P("ep", "tp"),
        P("ep", "tp"),
        P(None, "tp"),
        P("tp"),
        P("tp", None),
        P("ep", None),
        P(),
        P("ep", None, "tp"),
        P("ep", None, "tp"),
        P("ep", "tp", None),
        P("ep", None),
        P("ep", None),
    )
    out_specs = (P(("ep", "tp"), None), P("ep", "tp"))
    return jax.shard_map(
        on_device, mesh=mesh, in_specs=in_specs, out_specs=out_specs, check_vma=False
    )
```

```python
import functools

import jax
import jax.numpy as jnp
from jax import lax
from jax.experimental import pallas as pl
from jax.experimental.pallas import tpu as pltpu
from jax.sharding import PartitionSpec as P

eps_rms = 1e-06
eps_norm = 1e-05
MESH = pl.DeviceIdType.MESH
F32 = jnp.float32
BF16 = jnp.bfloat16

A2A_S, A2A_R, AGR_S, AGR_R, AGL_S, AGL_R, FWR_S, FWR_R, FWL_S, FWL_R = range(10)
S1R_S, S1R_R, S1L_S, S1L_R, S2R_S, S2R_R, S2L_S, S2L_R, RET_S, RET_R = range(10, 20)
A2P_S, A2P_R = 20, 21
HALO, STAT_P, STAT_M, STAT_O, ACT_P, ACT_M, ACT_O, WR, WL, WFR, WFL, YR, YL, YFR, YFL, WC = range(16)


NARROW = False


def layout_of(ep_count):
    if ep_count == 64:
        return 8, (0, 7, 2, 5, 3, 4, 1, 6), (0, 0, 0, 0, 0, 0, 1, 1), 2
    if ep_count == 32:
        return 8, (2, 0, 3, 1), (0, 1, 0, 1), 1
    if ep_count == 8 and NARROW:
        return 8, (0,), (0,), 1
    return 2, (2, 0, 3, 1), (0, 1, 0, 1), 1


def block_kernel(
    cfg,
    gain_hbm,
    ids_hbm,
    route_hbm,
    taps_hbm,
    ln_gain_hbm,
    moe_hbm,
    value_hbm,
    gate_hbm,
    w_out_hbm,
    w_gate_hbm,
    w_up_hbm,
    w_down_hbm,
    mixed,
    out,
    gain,
    ids_t,
    route_t,
    taps,
    ln_gain,
    moe_in,
    value,
    gate,
    w_out,
    wg,
    wu,
    wd,
    normed,
    send_full,
    send_part,
    xin,
    hid,
    part,
    s1r,
    s1l,
    s2r,
    s2l,
    ans,
    ret,
    tail,
    halo,
    gated,
    conv,
    stat,
    stat_in,
    act,
    act_in,
    total,
    w_sem,
    sems,
    msend,
    mrecv,
):
    nz, nyc, order, whole, per_chunk, cap = cfg
    ep = lax.axis_index("ep")
    x = lax.axis_index("tp")
    z = ep // nyc
    yc = ep % nyc
    xp, xm, xo = (x + 1) % 4, (x + 3) % 4, (x + 2) % 4
    n_ep = nz * nyc
    n_chunks = nz // per_chunk
    rows = per_chunk * nyc * cap
    half = rows // 2
    group = nyc * cap
    tokens, width = moe_in.shape
    quarter = width // 4
    whole_at = {p: sum(whole[:p]) for p in range(nz) if whole[p]}
    part_at = {p: p - sum(whole[:p]) for p in range(nz) if not whole[p]}
    own = order.index(0)

    barrier = pltpu.get_barrier_semaphore()

    def greet(j, c):
        pl.semaphore_signal(
            barrier, inc=1, device_id=((ep + j) % n_ep, x), device_id_type=MESH
        )
        return c

    lax.fori_loop(1, n_ep, greet, 0)
    for other in (xp, xm, xo):
        pl.semaphore_signal(barrier, inc=1, device_id=(ep, other), device_id_type=MESH)

    loads = [
        pltpu.make_async_copy(src, dst, w_sem.at[i])
        for i, (src, dst) in enumerate(
            (
                (moe_hbm, moe_in),
                (value_hbm, value),
                (gate_hbm, gate),
                (w_out_hbm, w_out.at[x]),
                (w_gate_hbm.at[0], wg),
                (w_up_hbm.at[0], wu),
                (w_down_hbm.at[0], wd),
                (ids_hbm, ids_t),
                (gain_hbm, gain),
                (route_hbm, route_t),
                (taps_hbm, taps),
                (ln_gain_hbm, ln_gain),
            )
        )
    ]
    for i in (7, 0, 8, 1, 2, 3, 9, 10, 11, 4, 5, 6):
        loads[i].start()

    def rdma(src, dst, row_s, row_r, k, to_ep, to_x):
        return pltpu.make_async_remote_copy(
            src_ref=src,
            dst_ref=dst,
            send_sem=sems.at[row_s, k],
            recv_sem=sems.at[row_r, k],
            device_id=(to_ep, to_x),
            device_id_type=MESH,
        )

    block = min(32, tokens)

    def norm_rows(i, c):
        at = pl.ds(pl.multiple_of(i * block, block), block)
        v = moe_in[at, :].astype(F32)
        scale = lax.rsqrt(jnp.sum(v * v, axis=1, keepdims=True) / width + eps_rms)
        y = (v * scale * gain[...]).astype(BF16)
        for q in range(4):
            normed[q, at, :] = y[:, q * quarter : (q + 1) * quarter]
        return c

    def place(e):
        dz = (e // nyc - z + nz) % nz
        pos = jnp.zeros_like(e)
        for p, d in enumerate(order):
            pos = jnp.where(dz == d, p, pos)
        return ((pos * nyc + e % nyc) * cap).astype(F32)

    with jax.named_scope("slots"):
        loads[7].wait()
        ti = lax.broadcasted_iota(jnp.int32, (tokens, tokens), 0)
        tj = lax.broadcasted_iota(jnp.int32, (tokens, tokens), 1)
        er = lax.broadcasted_iota(jnp.int32, (64, tokens), 0)
        e0r, e1r = ids_t[0:1, :], ids_t[1:2, :]
        hit0, hit1 = er == e0r, er == e1r
        mbr = jnp.where(hit0 | hit1, 1.0, 0.0).astype(BF16)
        before = jnp.where(ti < tj, 1.0, 0.0).astype(BF16)
        earlier_r = jnp.dot(mbr, before, preferred_element_type=F32)
        slot0r = place(e0r) + jnp.sum(jnp.where(hit0, earlier_r, 0.0), axis=0, keepdims=True)
        slot1r = place(e1r) + jnp.sum(jnp.where(hit1, earlier_r, 0.0), axis=0, keepdims=True)

    def pick_rows(start, count):
        at = (lax.broadcasted_iota(jnp.int32, (count, tokens), 0) + start).astype(F32)
        return jnp.where((at == slot0r) | (at == slot1r), 1.0, 0.0).astype(BF16)

    def fill(p):
        pick = pick_rows(p * group, group)
        if whole[p]:
            at = pl.ds(whole_at[p] * group, group)
            for q in range(4):
                send_full[q, at, :] = jnp.dot(
                    pick, normed[q], preferred_element_type=F32
                ).astype(BF16)
        else:
            at = pl.ds(part_at[p] * group, group)
            send_part[at, :] = jnp.dot(pick, normed[x], preferred_element_type=F32).astype(BF16)

    def send_rows(p):
        dz = order[p]
        k = p // per_chunk
        to_z = (z + dz) % nz

        def send(j, c):
            other = (yc + j) % nyc
            there = pl.ds(pl.multiple_of((p * nyc + yc) * cap, cap), cap)
            if whole[p]:
                here = pl.ds(pl.multiple_of((whole_at[p] * nyc + other) * cap, cap), cap)
                copy = rdma(
                    send_full.at[:, here, :],
                    xin.at[:, there, :],
                    A2A_S, A2A_R, k, to_z * nyc + other, x,
                )
            else:
                here = pl.ds(pl.multiple_of((part_at[p] * nyc + other) * cap, cap), cap)
                copy = rdma(
                    send_part.at[here, :],
                    xin.at[x, there, :],
                    A2P_S, A2P_R, k, to_z * nyc + other, x,
                )
            copy.start()
            return c

        lax.fori_loop(1 if dz == 0 else 0, nyc, send, 0)

    def fill_chunk(k):
        for p in range(k * per_chunk, (k + 1) * per_chunk):
            fill(p)

    def send_chunk(k):
        for p in range(k * per_chunk, (k + 1) * per_chunk):
            send_rows(p)

    mine = pl.ds(pl.multiple_of((own * nyc + yc) * cap, cap), cap)

    def keep_own():
        if whole[own]:
            here = pl.ds(pl.multiple_of((whole_at[own] * nyc + yc) * cap, cap), cap)
            for q in range(4):
                xin[q, mine, :] = send_full[q, here, :]
        else:
            here = pl.ds(pl.multiple_of((part_at[own] * nyc + yc) * cap, cap), cap)
            xin[x, mine, :] = send_part[here, :]

    def at_chunk(k):
        return pl.ds(k * rows, rows)

    def parts_of(k):
        n = sum(whole[k * per_chunk : (k + 1) * per_chunk]) * group
        return k * rows, n, k * rows + n, rows - n

    def less_own(k, is_whole):
        return cap if own // per_chunk == k and bool(whole[own]) == is_whole else 0

    def wait_in(k):
        w0, wn, g0, gn = parts_of(k)
        if wn:
            region = xin.at[:, pl.ds(w0, wn - less_own(k, True)), :]
            rdma(region, region, A2A_S, A2A_R, k, ep, xp).wait_recv()
        if gn:
            region = xin.at[x, pl.ds(g0, gn - less_own(k, False)), :]
            rdma(region, region, A2P_S, A2P_R, k, ep, xp).wait_recv()

    def gather_start(k):
        _, _, g0, gn = parts_of(k)
        if gn:
            region = xin.at[x, pl.ds(g0, gn), :]
            rdma(region, region, AGR_S, AGR_R, k, ep, xp).start()
            rdma(region, region, AGL_S, AGL_R, k, ep, xm).start()

    def gather_forward(k):
        _, _, g0, gn = parts_of(k)
        if gn:
            left = xin.at[xm, pl.ds(g0, gn), :]
            rdma(left, left, AGR_S, AGR_R, k, ep, xp).wait_recv()
            top = xin.at[xm, pl.ds(g0, gn // 2), :]
            rdma(top, top, FWR_S, FWR_R, k, ep, xp).start()
            right = xin.at[xp, pl.ds(g0, gn), :]
            rdma(right, right, AGL_S, AGL_R, k, ep, xm).wait_recv()
            low = xin.at[xp, pl.ds(g0 + gn // 2, gn // 2), :]
            rdma(low, low, FWL_S, FWL_R, k, ep, xm).start()

    def gather_done(k):
        _, _, g0, gn = parts_of(k)
        if gn:
            top = xin.at[xo, pl.ds(g0, gn // 2), :]
            low = xin.at[xo, pl.ds(g0 + gn // 2, gn // 2), :]
            rdma(top, top, FWR_S, FWR_R, k, ep, xp).wait_recv()
            rdma(low, low, FWL_S, FWL_R, k, ep, xm).wait_recv()

    hidden_dev = wg.shape[1]
    nb = min(256, hidden_dev)

    def compute(k):
        def up(n, c):
            cols = pl.ds(pl.multiple_of(n * nb, nb), nb)
            g = jnp.zeros((rows, nb), F32)
            u = jnp.zeros((rows, nb), F32)
            for q in range(4):
                xq = xin[q, at_chunk(k), :]
                ws = pl.ds(q * quarter, quarter)
                g = g + jnp.dot(xq, wg[ws, cols], preferred_element_type=F32)
                u = u + jnp.dot(xq, wu[ws, cols], preferred_element_type=F32)
            hid[:, cols] = (g / (1.0 + jnp.exp(-g)) * u).astype(BF16)
            return c

        lax.fori_loop(0, hidden_dev // nb, up, 0)

        def down(d):
            cols = pl.ds(pl.multiple_of(d * quarter, quarter), quarter)
            part[k, d] = jnp.dot(
                hid[...], wd[:, cols], preferred_element_type=F32
            ).astype(BF16)

        down(xo)
        down(xp)
        rdma(
            part.at[k, xo, pl.ds(0, half), :], s1r.at[k], S1R_S, S1R_R, k, ep, xp
        ).start()
        rdma(
            part.at[k, xo, pl.ds(half, half), :], s1l.at[k], S1L_S, S1L_R, k, ep, xm
        ).start()
        down(xm)
        down(x)

    def scatter_add(k):
        rdma(s1r.at[k], s1r.at[k], S1R_S, S1R_R, k, ep, xp).wait_recv()
        top = pl.ds(0, half)
        part[k, xp, top, :] = (
            part[k, xp, top, :].astype(F32) + s1r[k].astype(F32)
        ).astype(BF16)
        rdma(s1l.at[k], s1l.at[k], S1L_S, S1L_R, k, ep, xm).wait_recv()
        low = pl.ds(half, half)
        part[k, xm, low, :] = (
            part[k, xm, low, :].astype(F32) + s1l[k].astype(F32)
        ).astype(BF16)
        rdma(part.at[k, xp], s2r.at[k], S2R_S, S2R_R, k, ep, xp).start()
        rdma(part.at[k, xm], s2l.at[k], S2L_S, S2L_R, k, ep, xm).start()

    def give_back(k):
        rdma(s2r.at[k], s2r.at[k], S2R_S, S2R_R, k, ep, xp).wait_recv()
        rdma(s2l.at[k], s2l.at[k], S2L_S, S2L_R, k, ep, xm).wait_recv()
        sums = part[k, x].astype(F32) + s2r[k].astype(F32) + s2l[k].astype(F32)
        ans[at_chunk(k), :] = sums.astype(BF16)
        if k == own // per_chunk:
            ret[mine, :] = ans[mine, :]
        for p in range(k * per_chunk, (k + 1) * per_chunk):
            dz = order[p]
            to_z = (z - dz + nz) % nz

            def send(j, c, p=p, to_z=to_z):
                other = (yc + j) % nyc
                here = pl.ds(pl.multiple_of((p * nyc + other) * cap, cap), cap)
                there = pl.ds(pl.multiple_of((p * nyc + yc) * cap, cap), cap)
                rdma(
                    ans.at[here, :], ret.at[there, :], RET_S, RET_R, k,
                    to_z * nyc + other, x,
                ).start()
                return c

            lax.fori_loop(1 if dz == 0 else 0, nyc, send, 0)

    length, channels_dev = value.shape
    lane_groups = channels_dev // 128
    reach = taps.shape[0]
    m_rows = length // 4
    core = ep % 2
    partner = ep + 1 - 2 * core
    ny = nyc // 2
    yy = yc // 2
    y_up = z * nyc + (yy + 1) % ny * 2 + core
    y_down = z * nyc + (yy + ny - 1) % ny * 2 + core
    w_rows = channels_dev // nyc
    others = (xm, xp, xo)

    def mcopy(src, dst, row, to_ep, to_x):
        return pltpu.make_async_remote_copy(
            src_ref=src,
            dst_ref=dst,
            send_sem=msend.at[row],
            recv_sem=mrecv.at[row],
            device_id=(to_ep, to_x),
            device_id_type=MESH,
        )

    def mixer_gate():
        loads[1].wait()
        loads[2].wait()

        def rows_of(i, c):
            at = pl.ds(pl.multiple_of(i * 32, 32), 32)
            v = value[at, :].astype(F32)
            g = gate[at, :].astype(F32)
            y = (v * (1.0 / (1.0 + jnp.exp(-g)))).astype(BF16)
            wide = y.astype(F32)
            to = pl.ds(pl.multiple_of(i * 32 + 32, 32), 32)
            for h in range(lane_groups):
                gated[h, to, :] = wide[:, h * 128 : (h + 1) * 128]
            tail[...] = y
            return c

        lax.fori_loop(0, length // 32, rows_of, 0)

    def halo_send():
        mcopy(tail, halo, HALO, (ep + 1) % n_ep, x).start()

    def mixer_conv():
        mcopy(tail, halo, HALO, (ep + 1) % n_ep, x).wait_recv()
        before_first = jnp.where(ep == 0, 0.0, halo[...].astype(F32))
        for h in range(lane_groups):
            gated[h, 0:32, :] = before_first[:, h * 128 : (h + 1) * 128]
        cb = 64
        for h in range(lane_groups):
            lanes = slice(h * 128, (h + 1) * 128)

            def rows_of(i, c, h=h, lanes=lanes):
                base = pl.multiple_of(i * cb, cb)
                window = gated.at[h, pl.ds(base, cb + 32), :]
                acc = jnp.zeros((cb, 128), F32)
                for j in range(reach):
                    acc = acc + taps[j : j + 1, lanes] * window[32 - j : 32 - j + cb, :]
                conv[pl.ds(base, cb), lanes] = acc
                return c

            lax.fori_loop(0, length // cb, rows_of, 0)

        sb = 128
        lane = lax.broadcasted_iota(jnp.int32, (sb, 128), 1)
        for i in range(length // sb):
            c = conv[i * sb : (i + 1) * sb, :]
            total = jnp.sum(c, axis=1, keepdims=True)
            squares = jnp.sum(c * c, axis=1, keepdims=True)
            both = jnp.where(lane == 0, total, jnp.where(lane == 1, squares, 0.0))
            stat[:, i * sb : (i + 1) * sb] = both.T[0:8, :]
        for n, (row, to_x) in enumerate(((STAT_P, xp), (STAT_M, xm), (STAT_O, xo))):
            mcopy(stat, stat_in.at[n], row, ep, to_x).start()

    def mixer_out():
        for n, row in enumerate((STAT_P, STAT_M, STAT_O)):
            mcopy(stat, stat_in.at[n], row, ep, xp).wait_recv()
        sums = stat[...] + stat_in[0] + stat_in[1] + stat_in[2]
        channels = channels_dev * 4
        sb = 128
        for i in range(length // sb):
            at = slice(i * sb, (i + 1) * sb)
            mean = sums[0:1, at] / channels
            variance = sums[1:2, at] / channels - mean * mean
            scale = lax.rsqrt(variance + eps_norm)
            r = lax.broadcasted_iota(jnp.int32, (128, sb), 0)
            cols = jnp.where(r == 0, mean, jnp.where(r == 1, scale, 0.0)).T
            v = (conv[at, :] - cols[:, 0:1]) * cols[:, 1:2] * ln_gain[...]
            act[at, :] = (v / (1.0 + jnp.exp(-v))).astype(BF16)
        for row, to_x in ((ACT_P, xp), (ACT_M, xm), (ACT_O, xo)):
            at = pl.ds(pl.multiple_of(to_x * m_rows, m_rows), m_rows)
            mcopy(act.at[at, :], act_in.at[x], row, ep, to_x).start()
        act_in[x] = act[pl.ds(pl.multiple_of(x * m_rows, m_rows), m_rows), :]

    def w_start():
        loads[3].wait()
        sent = w_out.at[x, yy, core]
        mcopy(sent, sent, WR, ep, xp).start()
        mcopy(sent, sent, WL, ep, xm).start()

    def along_y(q):
        if ny > 1:
            sent = w_out.at[q, yy, core]
            mcopy(sent, sent, YR, y_up, x).start()
            mcopy(sent, sent, YL, y_down, x).start()

    def w_forward():
        left = w_out.at[xm, yy, core]
        mcopy(left, left, WR, ep, xp).wait_recv()
        top = w_out.at[xm, yy, core, pl.ds(0, w_rows // 2), :]
        mcopy(top, top, WFR, ep, xp).start()
        right = w_out.at[xp, yy, core]
        mcopy(right, right, WL, ep, xm).wait_recv()
        low = w_out.at[xp, yy, core, pl.ds(w_rows // 2, w_rows // 2), :]
        mcopy(low, low, WFL, ep, xm).start()
        along_y(xm)
        along_y(xp)

    def w_along_y():
        top = w_out.at[xo, yy, core, pl.ds(0, w_rows // 2), :]
        low = w_out.at[xo, yy, core, pl.ds(w_rows // 2, w_rows // 2), :]
        mcopy(top, top, WFR, ep, xp).wait_recv()
        mcopy(low, low, WFL, ep, xm).wait_recv()
        along_y(xo)

    def w_forward_y():
        if ny > 1:
            three = w_out.at[pl.ds(0, 3), yy, core]
            mcopy(three, three, YR, y_up, x).wait_recv()
            for q in others:
                top = w_out.at[q, (yy + ny - 1) % ny, core, pl.ds(0, w_rows // 2), :]
                mcopy(top, top, YFR, y_up, x).start()
            mcopy(three, three, YL, y_down, x).wait_recv()
            for q in others:
                low = w_out.at[q, (yy + 1) % ny, core, pl.ds(w_rows // 2, w_rows // 2), :]
                mcopy(low, low, YFL, y_down, x).start()

    def w_share():
        if ny > 1:
            three = w_out.at[pl.ds(0, 3), yy, core, pl.ds(0, w_rows // 2), :]
            mcopy(three, three, YFR, y_up, x).wait_recv()
            mcopy(three, three, YFL, y_down, x).wait_recv()
        for q in others:
            sent = w_out.at[q, :, core]
            mcopy(sent, sent, WC, partner, x).start()

    def mixer_project():
        for row, q in ((ACT_P, xm), (ACT_M, xp), (ACT_O, xo)):
            mcopy(act_in.at[q], act_in.at[q], row, ep, xp).wait_recv()
        theirs = w_out.at[pl.ds(0, 3), :, 1 - core]
        mcopy(theirs, theirs, WC, partner, x).wait_recv()

        def project(n, c):
            cols = pl.ds(pl.multiple_of(n * 256, 256), 256)
            sums = jnp.zeros((m_rows, 256), F32)
            for q in range(4):
                w = w_out[q, :, :, :, cols].reshape(channels_dev, 256)
                sums = sums + jnp.dot(act_in[q], w, preferred_element_type=F32)
            mixed[:, cols] = sums.astype(BF16)
            return c

        lax.fori_loop(0, width // 256, project, 0)

    def combine(k):
        region = ret.at[pl.ds(k * rows, rows - less_own(k, bool(whole[own]))), :]
        rdma(region, region, RET_S, RET_R, k, ep, xp).wait_recv()
        slot0c, slot1c = columns[:, 0:1], columns[:, 1:2]
        at = (lax.broadcasted_iota(jnp.int32, (tokens, rows), 1) + k * rows).astype(F32)
        w = jnp.where(at == slot0c, columns[:, 2:3], 0.0)
        w = w + jnp.where(at == slot1c, columns[:, 3:4], 0.0)
        high = w.astype(BF16)
        low = (w - high.astype(F32)).astype(BF16)
        got = ret[at_chunk(k), :]
        sums = jnp.dot(high, got, preferred_element_type=F32)
        sums = sums + jnp.dot(low, got, preferred_element_type=F32)
        total[...] = total[...] + sums

    def run(step, *k):
        if k and k[0] >= n_chunks:
            return
        with jax.named_scope(step.__name__ + "".join(f"#{i}" for i in k)):
            step(*k)

    with jax.named_scope("norm"):
        loads[0].wait()
        loads[8].wait()
        lax.fori_loop(0, tokens // block, norm_rows, 0)
    run(fill_chunk, 0)
    run(mixer_gate)
    with jax.named_scope("barrier_wait"):
        pl.semaphore_wait(barrier, n_ep - 1 + 3)
    halo_send()
    run(send_chunk, 0)
    run(w_start)
    for k in range(1, n_chunks):
        run(fill_chunk, k)
    keep_own()
    loads[9].wait()
    turn = lax.broadcasted_iota(jnp.int32, (128, tokens), 0)
    table = jnp.where(turn == 0, slot0r, jnp.where(turn == 1, slot1r, 0.0))
    table = jnp.where(turn == 2, route_t[0:1, :], table)
    table = jnp.where(turn == 3, route_t[1:2, :], table)
    columns = table.T

    loads[10].wait()
    loads[11].wait()
    total[...] = jnp.zeros_like(total)
    run(send_chunk, 1)
    run(send_chunk, 2)
    run(mixer_conv)
    run(w_forward)
    run(wait_in, 0)
    run(gather_start, 0)
    run(mixer_out)
    run(w_along_y)
    for load in loads[4:7]:
        load.wait()
    run(gather_forward, 0)
    run(send_chunk, 3)
    run(wait_in, 1)
    run(gather_start, 1)
    run(gather_done, 0)
    run(compute, 0)
    run(gather_forward, 1)
    run(wait_in, 2)
    run(gather_start, 2)
    run(gather_done, 1)
    run(compute, 1)
    run(gather_forward, 2)
    run(scatter_add, 1)
    run(w_forward_y)
    run(gather_done, 2)
    run(compute, 2)
    run(wait_in, 3)
    run(compute, 3)
    run(give_back, 1)
    run(scatter_add, 2)
    run(scatter_add, 3)
    run(w_share)
    run(give_back, 2)
    run(scatter_add, 0)
    run(give_back, 3)
    run(combine, 1)
    run(give_back, 0)
    run(mixer_project)
    run(combine, 2)
    run(combine, 3)
    run(combine, 0)
    out[...] = total[...].astype(BF16)

    for k in range(n_chunks):
        w0, wn, g0, gn = parts_of(k)
        if wn:
            region = send_full.at[:, pl.ds(0, wn - less_own(k, True)), :]
            rdma(region, region, A2A_S, A2A_R, k, ep, xp).wait_send()
        if gn:
            region = send_part.at[pl.ds(0, gn - less_own(k, False)), :]
            rdma(region, region, A2P_S, A2P_R, k, ep, xp).wait_send()
            region = xin.at[x, pl.ds(g0, gn), :]
            rdma(region, region, AGR_S, AGR_R, k, ep, xp).wait_send()
            rdma(region, region, AGL_S, AGL_R, k, ep, xm).wait_send()
            region = xin.at[x, pl.ds(g0, gn // 2), :]
            rdma(region, region, FWR_S, FWR_R, k, ep, xp).wait_send()
            rdma(region, region, FWL_S, FWL_R, k, ep, xm).wait_send()
        back = ans.at[pl.ds(k * rows, rows - less_own(k, bool(whole[own]))), :]
        rdma(s1r.at[k], s1r.at[k], S1R_S, S1R_R, k, ep, xp).wait_send()
        rdma(s1l.at[k], s1l.at[k], S1L_S, S1L_R, k, ep, xm).wait_send()
        rdma(s2r.at[k], s2r.at[k], S2R_S, S2R_R, k, ep, xp).wait_send()
        rdma(s2l.at[k], s2l.at[k], S2L_S, S2L_R, k, ep, xm).wait_send()
        rdma(back, back, RET_S, RET_R, k, ep, xp).wait_send()
    mcopy(tail, tail, HALO, ep, xp).wait_send()
    for row in (STAT_P, STAT_M, STAT_O):
        mcopy(stat, stat, row, ep, xp).wait_send()
    for row in (ACT_P, ACT_M, ACT_O):
        mcopy(act_in.at[0], act_in.at[0], row, ep, xp).wait_send()
    sent = w_out.at[x, yy, core]
    mcopy(sent, sent, WR, ep, xp).wait_send()
    mcopy(sent, sent, WL, ep, xp).wait_send()
    sent = w_out.at[x, yy, core, pl.ds(0, w_rows // 2), :]
    mcopy(sent, sent, WFR, ep, xp).wait_send()
    mcopy(sent, sent, WFL, ep, xp).wait_send()
    if ny > 1:
        sent = w_out.at[pl.ds(0, 3), yy, core]
        mcopy(sent, sent, YR, y_up, x).wait_send()
        mcopy(sent, sent, YL, y_down, x).wait_send()
        sent = w_out.at[pl.ds(0, 3), yy, core, pl.ds(0, w_rows // 2), :]
        mcopy(sent, sent, YFR, y_up, x).wait_send()
        mcopy(sent, sent, YFL, y_down, x).wait_send()
    sent = w_out.at[pl.ds(0, 3), :, core]
    mcopy(sent, sent, WC, partner, x).wait_send()


def on_device(
    glu_value,
    glu_gate,
    conv_kernel,
    ln_gain,
    out_weight,
    moe_input,
    moe_gain,
    gate_weight,
    up_weight,
    down_weight,
    expert_ids,
    route_weight,
):
    tokens, width = moe_input.shape
    length, channels_dev = glu_value.shape
    ep_count = lax.axis_size("ep")
    nyc, order, whole, per_chunk = layout_of(ep_count)
    nz = ep_count // nyc
    cap = 16
    hidden_dev = gate_weight.shape[2]
    quarter = width // 4
    n_chunks = nz // per_chunk
    rows = per_chunk * nyc * cap
    slots = ep_count * cap
    vmem = pl.BlockSpec(memory_space=pltpu.VMEM)
    hbm = pl.BlockSpec(memory_space=pl.ANY)
    n_whole = sum(whole) * nyc * cap
    cfg = (nz, nyc, order, whole, per_chunk, cap)
    return pl.pallas_call(
        functools.partial(block_kernel, cfg),
        out_shape=(
            pltpu.VMEM((length // 4, width), BF16),
            pltpu.VMEM((tokens, quarter), BF16),
        ),
        in_specs=[hbm] * 12,
        out_specs=(vmem, vmem),
        scratch_shapes=[
            pltpu.VMEM((1, width), F32),
            pltpu.VMEM(expert_ids.shape[::-1], jnp.int32),
            pltpu.VMEM(route_weight.shape[::-1], F32),
            pltpu.VMEM(conv_kernel.shape, F32),
            pltpu.VMEM((1, channels_dev), F32),
            pltpu.VMEM((tokens, width), BF16),
            pltpu.VMEM((length, channels_dev), BF16),
            pltpu.VMEM((length, channels_dev), BF16),
            pltpu.VMEM((4, nyc // 2, 2, channels_dev // nyc, width), BF16),
            pltpu.VMEM((width, hidden_dev), BF16),
            pltpu.VMEM((width, hidden_dev), BF16),
            pltpu.VMEM((hidden_dev, width), BF16),
            pltpu.VMEM((4, tokens, quarter), BF16),
            pltpu.VMEM((4, max(n_whole, 16), quarter), BF16),
            pltpu.VMEM((max(slots - n_whole, 16), quarter), BF16),
            pltpu.VMEM((4, slots, quarter), BF16),
            pltpu.VMEM((rows, hidden_dev), BF16),
            pltpu.VMEM((n_chunks, 4, rows, quarter), BF16),
            pltpu.VMEM((n_chunks, rows // 2, quarter), BF16),
            pltpu.VMEM((n_chunks, rows // 2, quarter), BF16),
            pltpu.VMEM((n_chunks, rows, quarter), BF16),
            pltpu.VMEM((n_chunks, rows, quarter), BF16),
            pltpu.VMEM((slots, quarter), BF16),
            pltpu.VMEM((slots, quarter), BF16),
            pltpu.VMEM((32, channels_dev), BF16),
            pltpu.VMEM((32, channels_dev), BF16),
            pltpu.VMEM((channels_dev // 128, length + 32, 128), F32),
            pltpu.VMEM((length, channels_dev), F32),
            pltpu.VMEM((8, length), F32),
            pltpu.VMEM((3, 8, length), F32),
            pltpu.VMEM((length, channels_dev), BF16),
            pltpu.VMEM((4, length // 4, channels_dev), BF16),
            pltpu.VMEM((tokens, quarter), F32),
            pltpu.SemaphoreType.DMA((12,)),
            pltpu.SemaphoreType.DMA((22, n_chunks)),
            pltpu.SemaphoreType.DMA((16,)),
            pltpu.SemaphoreType.DMA((16,)),
        ],
        compiler_params=pltpu.CompilerParams(
            collective_id=0, has_side_effects=True, vmem_limit_bytes=60 * 1024 * 1024
        ),
        name="block",
    )(
        moe_gain[None, :],
        expert_ids.T,
        route_weight.T,
        conv_kernel,
        ln_gain[None, :],
        moe_input,
        glu_value,
        glu_gate,
        out_weight.reshape(nyc // 2, 2, channels_dev // nyc, width),
        gate_weight,
        up_weight,
        down_weight,
    )


def solution(mesh):
    in_specs = (
        P("ep", "tp"),
        P("ep", "tp"),
        P(None, "tp"),
        P("tp"),
        P("tp", None),
        P("ep", None),
        P(),
        P("ep", None, "tp"),
        P("ep", None, "tp"),
        P("ep", "tp", None),
        P("ep", None),
        P("ep", None),
    )
    out_specs = (P(("ep", "tp"), None), P("ep", "tp"))
    return jax.shard_map(
        on_device, mesh=mesh, in_specs=in_specs, out_specs=out_specs, check_vma=False
    )
```

```python
import functools

import jax
import jax.numpy as jnp
from jax import lax
from jax.experimental import pallas as pl
from jax.experimental.pallas import tpu as pltpu
from jax.sharding import PartitionSpec as P

eps_rms = 1e-06
eps_norm = 1e-05
MESH = pl.DeviceIdType.MESH
F32 = jnp.float32
BF16 = jnp.bfloat16

A2A_S, A2A_R, AGR_S, AGR_R, AGL_S, AGL_R, FWR_S, FWR_R, FWL_S, FWL_R = range(10)
S1R_S, S1R_R, S1L_S, S1L_R, S2R_S, S2R_R, S2L_S, S2L_R, RET_S, RET_R = range(10, 20)
A2P_S, A2P_R = 20, 21
HALO, STAT_P, STAT_M, STAT_O, ACT_P, ACT_M, ACT_O, WR, WL, WFR, WFL, YR, YL, YFR, YFL, WC = range(16)


NARROW = False


def layout_of(ep_count):
    if ep_count == 64:
        return 8, (0, 7, 2, 5, 3, 4, 1, 6), (0, 0, 0, 0, 0, 0, 1, 1), 2
    if ep_count == 32:
        return 8, (2, 0, 3, 1), (0, 1, 0, 1), 1
    if ep_count == 8 and NARROW:
        return 8, (0,), (0,), 1
    return 2, (2, 0, 3, 1), (0, 1, 0, 1), 1


def block_kernel(
    cfg,
    gain_hbm,
    ids_hbm,
    route_hbm,
    taps_hbm,
    ln_gain_hbm,
    moe_hbm,
    value_hbm,
    gate_hbm,
    w_out_hbm,
    w_gate_hbm,
    w_up_hbm,
    w_down_hbm,
    mixed,
    out,
    gain,
    ids_t,
    route_t,
    taps,
    ln_gain,
    moe_in,
    value,
    gate,
    w_out,
    wg,
    wu,
    wd,
    normed,
    send_full,
    send_part,
    xin,
    hid,
    part,
    s1r,
    s1l,
    s2r,
    s2l,
    ans,
    ret,
    tail,
    halo,
    gated,
    conv,
    stat,
    stat_in,
    act,
    act_in,
    total,
    w_sem,
    sems,
    msend,
    mrecv,
):
    nz, nyc, order, whole, per_chunk, cap = cfg
    ep = lax.axis_index("ep")
    x = lax.axis_index("tp")
    z = ep // nyc
    yc = ep % nyc
    xp, xm, xo = (x + 1) % 4, (x + 3) % 4, (x + 2) % 4
    n_ep = nz * nyc
    n_chunks = nz // per_chunk
    rows = per_chunk * nyc * cap
    half = rows // 2
    group = nyc * cap
    tokens, width = moe_in.shape
    quarter = width // 4
    whole_at = {p: sum(whole[:p]) for p in range(nz) if whole[p]}
    part_at = {p: p - sum(whole[:p]) for p in range(nz) if not whole[p]}
    own = order.index(0)

    barrier = pltpu.get_barrier_semaphore()

    def greet(j, c):
        pl.semaphore_signal(
            barrier, inc=1, device_id=((ep + j) % n_ep, x), device_id_type=MESH
        )
        return c

    lax.fori_loop(1, n_ep, greet, 0, unroll=9 if n_ep == 64 else 1)
    for other in (xp, xm, xo):
        pl.semaphore_signal(barrier, inc=1, device_id=(ep, other), device_id_type=MESH)

    loads = [
        pltpu.make_async_copy(src, dst, w_sem.at[i])
        for i, (src, dst) in enumerate(
            (
                (moe_hbm, moe_in),
                (value_hbm, value),
                (gate_hbm, gate),
                (w_out_hbm, w_out.at[x]),
                (w_gate_hbm.at[0], wg),
                (w_up_hbm.at[0], wu),
                (w_down_hbm.at[0], wd),
                (ids_hbm, ids_t),
                (gain_hbm, gain),
                (route_hbm, route_t),
                (taps_hbm, taps),
                (ln_gain_hbm, ln_gain),
            )
        )
    ]
    for i in (7, 0, 8, 1, 2, 3, 9, 10, 11, 4, 5, 6):
        loads[i].start()

    def rdma(src, dst, row_s, row_r, k, to_ep, to_x):
        return pltpu.make_async_remote_copy(
            src_ref=src,
            dst_ref=dst,
            send_sem=sems.at[row_s, k],
            recv_sem=sems.at[row_r, k],
            device_id=(to_ep, to_x),
            device_id_type=MESH,
        )

    block = min(32, tokens)

    def norm_rows(i, c):
        at = pl.ds(pl.multiple_of(i * block, block), block)
        v = moe_in[at, :].astype(F32)
        scale = lax.rsqrt(jnp.sum(v * v, axis=1, keepdims=True) / width + eps_rms)
        y = (v * scale * gain[...]).astype(BF16)
        for q in range(4):
            normed[q, at, :] = y[:, q * quarter : (q + 1) * quarter]
        return c

    def place(e):
        dz = (e // nyc - z + nz) % nz
        pos = jnp.zeros_like(e)
        for p, d in enumerate(order):
            pos = jnp.where(dz == d, p, pos)
        return ((pos * nyc + e % nyc) * cap).astype(F32)

    with jax.named_scope("slots"):
        loads[7].wait()
        ti = lax.broadcasted_iota(jnp.int32, (tokens, tokens), 0)
        tj = lax.broadcasted_iota(jnp.int32, (tokens, tokens), 1)
        er = lax.broadcasted_iota(jnp.int32, (64, tokens), 0)
        e0r, e1r = ids_t[0:1, :], ids_t[1:2, :]
        hit0, hit1 = er == e0r, er == e1r
        mbr = jnp.where(hit0 | hit1, 1.0, 0.0).astype(BF16)
        before = jnp.where(ti < tj, 1.0, 0.0).astype(BF16)
        earlier_r = jnp.dot(mbr, before, preferred_element_type=F32)
        slot0r = place(e0r) + jnp.sum(jnp.where(hit0, earlier_r, 0.0), axis=0, keepdims=True)
        slot1r = place(e1r) + jnp.sum(jnp.where(hit1, earlier_r, 0.0), axis=0, keepdims=True)

    def pick_rows(start, count):
        at = (lax.broadcasted_iota(jnp.int32, (count, tokens), 0) + start).astype(F32)
        return jnp.where((at == slot0r) | (at == slot1r), 1.0, 0.0).astype(BF16)

    def fill(p):
        pick = pick_rows(p * group, group)
        if whole[p]:
            at = pl.ds(whole_at[p] * group, group)
            for q in range(4):
                send_full[q, at, :] = jnp.dot(
                    pick, normed[q], preferred_element_type=F32
                ).astype(BF16)
        else:
            at = pl.ds(part_at[p] * group, group)
            send_part[at, :] = jnp.dot(pick, normed[x], preferred_element_type=F32).astype(BF16)

    def send_rows(p):
        dz = order[p]
        k = p // per_chunk
        to_z = (z + dz) % nz

        def send(j, c):
            other = (yc + j) % nyc
            there = pl.ds(pl.multiple_of((p * nyc + yc) * cap, cap), cap)
            if whole[p]:
                here = pl.ds(pl.multiple_of((whole_at[p] * nyc + other) * cap, cap), cap)
                copy = rdma(
                    send_full.at[:, here, :],
                    xin.at[:, there, :],
                    A2A_S, A2A_R, k, to_z * nyc + other, x,
                )
            else:
                here = pl.ds(pl.multiple_of((part_at[p] * nyc + other) * cap, cap), cap)
                copy = rdma(
                    send_part.at[here, :],
                    xin.at[x, there, :],
                    A2P_S, A2P_R, k, to_z * nyc + other, x,
                )
            copy.start()
            return c

        lax.fori_loop(1 if dz == 0 else 0, nyc, send, 0)

    def fill_chunk(k):
        for p in range(k * per_chunk, (k + 1) * per_chunk):
            fill(p)

    def send_chunk(k):
        for p in range(k * per_chunk, (k + 1) * per_chunk):
            send_rows(p)

    mine = pl.ds(pl.multiple_of((own * nyc + yc) * cap, cap), cap)

    def keep_own():
        if whole[own]:
            here = pl.ds(pl.multiple_of((whole_at[own] * nyc + yc) * cap, cap), cap)
            for q in range(4):
                xin[q, mine, :] = send_full[q, here, :]
        else:
            here = pl.ds(pl.multiple_of((part_at[own] * nyc + yc) * cap, cap), cap)
            xin[x, mine, :] = send_part[here, :]

    def at_chunk(k):
        return pl.ds(k * rows, rows)

    def parts_of(k):
        n = sum(whole[k * per_chunk : (k + 1) * per_chunk]) * group
        return k * rows, n, k * rows + n, rows - n

    def less_own(k, is_whole):
        return cap if own // per_chunk == k and bool(whole[own]) == is_whole else 0

    def wait_in(k):
        w0, wn, g0, gn = parts_of(k)
        if wn:
            region = xin.at[:, pl.ds(w0, wn - less_own(k, True)), :]
            rdma(region, region, A2A_S, A2A_R, k, ep, xp).wait_recv()
        if gn:
            region = xin.at[x, pl.ds(g0, gn - less_own(k, False)), :]
            rdma(region, region, A2P_S, A2P_R, k, ep, xp).wait_recv()

    def gather_start(k):
        _, _, g0, gn = parts_of(k)
        if gn:
            region = xin.at[x, pl.ds(g0, gn), :]
            rdma(region, region, AGR_S, AGR_R, k, ep, xp).start()
            rdma(region, region, AGL_S, AGL_R, k, ep, xm).start()

    def gather_forward(k):
        _, _, g0, gn = parts_of(k)
        if gn:
            left = xin.at[xm, pl.ds(g0, gn), :]
            rdma(left, left, AGR_S, AGR_R, k, ep, xp).wait_recv()
            top = xin.at[xm, pl.ds(g0, gn // 2), :]
            rdma(top, top, FWR_S, FWR_R, k, ep, xp).start()
            right = xin.at[xp, pl.ds(g0, gn), :]
            rdma(right, right, AGL_S, AGL_R, k, ep, xm).wait_recv()
            low = xin.at[xp, pl.ds(g0 + gn // 2, gn // 2), :]
            rdma(low, low, FWL_S, FWL_R, k, ep, xm).start()

    def gather_done(k):
        _, _, g0, gn = parts_of(k)
        if gn:
            top = xin.at[xo, pl.ds(g0, gn // 2), :]
            low = xin.at[xo, pl.ds(g0 + gn // 2, gn // 2), :]
            rdma(top, top, FWR_S, FWR_R, k, ep, xp).wait_recv()
            rdma(low, low, FWL_S, FWL_R, k, ep, xm).wait_recv()

    hidden_dev = wg.shape[1]
    nb = min(256, hidden_dev)

    def compute(k):
        def up(n, c):
            cols = pl.ds(pl.multiple_of(n * nb, nb), nb)
            g = jnp.zeros((rows, nb), F32)
            u = jnp.zeros((rows, nb), F32)
            for q in range(4):
                xq = xin[q, at_chunk(k), :]
                ws = pl.ds(q * quarter, quarter)
                g = g + jnp.dot(xq, wg[ws, cols], preferred_element_type=F32)
                u = u + jnp.dot(xq, wu[ws, cols], preferred_element_type=F32)
            hid[:, cols] = (g / (1.0 + jnp.exp(-g)) * u).astype(BF16)
            return c

        lax.fori_loop(0, hidden_dev // nb, up, 0)

        def down(d):
            cols = pl.ds(pl.multiple_of(d * quarter, quarter), quarter)
            part[k, d] = jnp.dot(
                hid[...], wd[:, cols], preferred_element_type=F32
            ).astype(BF16)

        down(xo)
        down(xp)
        rdma(
            part.at[k, xo, pl.ds(0, half), :], s1r.at[k], S1R_S, S1R_R, k, ep, xp
        ).start()
        rdma(
            part.at[k, xo, pl.ds(half, half), :], s1l.at[k], S1L_S, S1L_R, k, ep, xm
        ).start()
        down(xm)
        down(x)

    def scatter_add(k):
        rdma(s1r.at[k], s1r.at[k], S1R_S, S1R_R, k, ep, xp).wait_recv()
        top = pl.ds(0, half)
        part[k, xp, top, :] = (
            part[k, xp, top, :].astype(F32) + s1r[k].astype(F32)
        ).astype(BF16)
        rdma(s1l.at[k], s1l.at[k], S1L_S, S1L_R, k, ep, xm).wait_recv()
        low = pl.ds(half, half)
        part[k, xm, low, :] = (
            part[k, xm, low, :].astype(F32) + s1l[k].astype(F32)
        ).astype(BF16)
        rdma(part.at[k, xp], s2r.at[k], S2R_S, S2R_R, k, ep, xp).start()
        rdma(part.at[k, xm], s2l.at[k], S2L_S, S2L_R, k, ep, xm).start()

    def give_back(k):
        rdma(s2r.at[k], s2r.at[k], S2R_S, S2R_R, k, ep, xp).wait_recv()
        rdma(s2l.at[k], s2l.at[k], S2L_S, S2L_R, k, ep, xm).wait_recv()
        sums = part[k, x].astype(F32) + s2r[k].astype(F32) + s2l[k].astype(F32)
        ans[at_chunk(k), :] = sums.astype(BF16)
        if k == own // per_chunk:
            ret[mine, :] = ans[mine, :]
        for p in range(k * per_chunk, (k + 1) * per_chunk):
            dz = order[p]
            to_z = (z - dz + nz) % nz

            def send(j, c, p=p, to_z=to_z):
                other = (yc + j) % nyc
                here = pl.ds(pl.multiple_of((p * nyc + other) * cap, cap), cap)
                there = pl.ds(pl.multiple_of((p * nyc + yc) * cap, cap), cap)
                rdma(
                    ans.at[here, :], ret.at[there, :], RET_S, RET_R, k,
                    to_z * nyc + other, x,
                ).start()
                return c

            lax.fori_loop(1 if dz == 0 else 0, nyc, send, 0)

    length, channels_dev = value.shape
    lane_groups = channels_dev // 128
    reach = taps.shape[0]
    m_rows = length // 4
    core = ep % 2
    partner = ep + 1 - 2 * core
    ny = nyc // 2
    yy = yc // 2
    y_up = z * nyc + (yy + 1) % ny * 2 + core
    y_down = z * nyc + (yy + ny - 1) % ny * 2 + core
    w_rows = channels_dev // nyc
    others = (xm, xp, xo)

    def mcopy(src, dst, row, to_ep, to_x):
        return pltpu.make_async_remote_copy(
            src_ref=src,
            dst_ref=dst,
            send_sem=msend.at[row],
            recv_sem=mrecv.at[row],
            device_id=(to_ep, to_x),
            device_id_type=MESH,
        )

    def mixer_gate():
        loads[1].wait()
        loads[2].wait()

        def rows_of(i, c):
            at = pl.ds(pl.multiple_of(i * 32, 32), 32)
            v = value[at, :].astype(F32)
            g = gate[at, :].astype(F32)
            y = (v * (1.0 / (1.0 + jnp.exp(-g)))).astype(BF16)
            wide = y.astype(F32)
            to = pl.ds(pl.multiple_of(i * 32 + 32, 32), 32)
            for h in range(lane_groups):
                gated[h, to, :] = wide[:, h * 128 : (h + 1) * 128]
            tail[...] = y
            return c

        lax.fori_loop(0, length // 32, rows_of, 0)

    def halo_send():
        mcopy(tail, halo, HALO, (ep + 1) % n_ep, x).start()

    def mixer_conv():
        mcopy(tail, halo, HALO, (ep + 1) % n_ep, x).wait_recv()
        before_first = jnp.where(ep == 0, 0.0, halo[...].astype(F32))
        for h in range(lane_groups):
            gated[h, 0:32, :] = before_first[:, h * 128 : (h + 1) * 128]
        cb = 64
        for h in range(lane_groups):
            lanes = slice(h * 128, (h + 1) * 128)

            def rows_of(i, c, h=h, lanes=lanes):
                base = pl.multiple_of(i * cb, cb)
                window = gated.at[h, pl.ds(base, cb + 32), :]
                acc = jnp.zeros((cb, 128), F32)
                for j in range(reach):
                    acc = acc + taps[j : j + 1, lanes] * window[32 - j : 32 - j + cb, :]
                conv[pl.ds(base, cb), lanes] = acc
                return c

            lax.fori_loop(0, length // cb, rows_of, 0)

        sb = 128
        lane = lax.broadcasted_iota(jnp.int32, (sb, 128), 1)
        for i in range(length // sb):
            c = conv[i * sb : (i + 1) * sb, :]
            total = jnp.sum(c, axis=1, keepdims=True)
            squares = jnp.sum(c * c, axis=1, keepdims=True)
            both = jnp.where(lane == 0, total, jnp.where(lane == 1, squares, 0.0))
            stat[:, i * sb : (i + 1) * sb] = both.T[0:8, :]
        for n, (row, to_x) in enumerate(((STAT_P, xp), (STAT_M, xm), (STAT_O, xo))):
            mcopy(stat, stat_in.at[n], row, ep, to_x).start()

    def mixer_out():
        for n, row in enumerate((STAT_P, STAT_M, STAT_O)):
            mcopy(stat, stat_in.at[n], row, ep, xp).wait_recv()
        sums = stat[...] + stat_in[0] + stat_in[1] + stat_in[2]
        channels = channels_dev * 4
        sb = 128
        for i in range(length // sb):
            at = slice(i * sb, (i + 1) * sb)
            mean = sums[0:1, at] / channels
            variance = sums[1:2, at] / channels - mean * mean
            scale = lax.rsqrt(variance + eps_norm)
            r = lax.broadcasted_iota(jnp.int32, (128, sb), 0)
            cols = jnp.where(r == 0, mean, jnp.where(r == 1, scale, 0.0)).T
            v = (conv[at, :] - cols[:, 0:1]) * cols[:, 1:2] * ln_gain[...]
            act[at, :] = (v / (1.0 + jnp.exp(-v))).astype(BF16)
        for row, to_x in ((ACT_P, xp), (ACT_M, xm), (ACT_O, xo)):
            at = pl.ds(pl.multiple_of(to_x * m_rows, m_rows), m_rows)
            mcopy(act.at[at, :], act_in.at[x], row, ep, to_x).start()
        act_in[x] = act[pl.ds(pl.multiple_of(x * m_rows, m_rows), m_rows), :]

    def w_start():
        loads[3].wait()
        sent = w_out.at[x, yy, core]
        mcopy(sent, sent, WR, ep, xp).start()
        mcopy(sent, sent, WL, ep, xm).start()

    def along_y(q):
        if ny > 1:
            sent = w_out.at[q, yy, core]
            mcopy(sent, sent, YR, y_up, x).start()
            mcopy(sent, sent, YL, y_down, x).start()

    def w_forward():
        left = w_out.at[xm, yy, core]
        mcopy(left, left, WR, ep, xp).wait_recv()
        top = w_out.at[xm, yy, core, pl.ds(0, w_rows // 2), :]
        mcopy(top, top, WFR, ep, xp).start()
        right = w_out.at[xp, yy, core]
        mcopy(right, right, WL, ep, xm).wait_recv()
        low = w_out.at[xp, yy, core, pl.ds(w_rows // 2, w_rows // 2), :]
        mcopy(low, low, WFL, ep, xm).start()
        along_y(xm)
        along_y(xp)

    def w_along_y():
        top = w_out.at[xo, yy, core, pl.ds(0, w_rows // 2), :]
        low = w_out.at[xo, yy, core, pl.ds(w_rows // 2, w_rows // 2), :]
        mcopy(top, top, WFR, ep, xp).wait_recv()
        mcopy(low, low, WFL, ep, xm).wait_recv()
        along_y(xo)

    def w_forward_y():
        if ny > 1:
            three = w_out.at[pl.ds(0, 3), yy, core]
            mcopy(three, three, YR, y_up, x).wait_recv()
            for q in others:
                top = w_out.at[q, (yy + ny - 1) % ny, core, pl.ds(0, w_rows // 2), :]
                mcopy(top, top, YFR, y_up, x).start()
            mcopy(three, three, YL, y_down, x).wait_recv()
            for q in others:
                low = w_out.at[q, (yy + 1) % ny, core, pl.ds(w_rows // 2, w_rows // 2), :]
                mcopy(low, low, YFL, y_down, x).start()

    def w_share():
        if ny > 1:
            three = w_out.at[pl.ds(0, 3), yy, core, pl.ds(0, w_rows // 2), :]
            mcopy(three, three, YFR, y_up, x).wait_recv()
            mcopy(three, three, YFL, y_down, x).wait_recv()
        for q in others:
            sent = w_out.at[q, :, core]
            mcopy(sent, sent, WC, partner, x).start()

    def mixer_project():
        for row, q in ((ACT_P, xm), (ACT_M, xp), (ACT_O, xo)):
            mcopy(act_in.at[q], act_in.at[q], row, ep, xp).wait_recv()
        theirs = w_out.at[pl.ds(0, 3), :, 1 - core]
        mcopy(theirs, theirs, WC, partner, x).wait_recv()

        def project(n, c):
            cols = pl.ds(pl.multiple_of(n * 256, 256), 256)
            sums = jnp.zeros((m_rows, 256), F32)
            for q in range(4):
                w = w_out[q, :, :, :, cols].reshape(channels_dev, 256)
                sums = sums + jnp.dot(act_in[q], w, preferred_element_type=F32)
            mixed[:, cols] = sums.astype(BF16)
            return c

        lax.fori_loop(0, width // 256, project, 0)

    def combine(k):
        region = ret.at[pl.ds(k * rows, rows - less_own(k, bool(whole[own]))), :]
        rdma(region, region, RET_S, RET_R, k, ep, xp).wait_recv()
        slot0c, slot1c = columns[:, 0:1], columns[:, 1:2]
        at = (lax.broadcasted_iota(jnp.int32, (tokens, rows), 1) + k * rows).astype(F32)
        w = jnp.where(at == slot0c, columns[:, 2:3], 0.0)
        w = w + jnp.where(at == slot1c, columns[:, 3:4], 0.0)
        high = w.astype(BF16)
        low = (w - high.astype(F32)).astype(BF16)
        got = ret[at_chunk(k), :]
        sums = jnp.dot(high, got, preferred_element_type=F32)
        sums = sums + jnp.dot(low, got, preferred_element_type=F32)
        total[...] = total[...] + sums

    def run(step, *k):
        if k and k[0] >= n_chunks:
            return
        with jax.named_scope(step.__name__ + "".join(f"#{i}" for i in k)):
            step(*k)

    with jax.named_scope("norm"):
        loads[0].wait()
        loads[8].wait()
        lax.fori_loop(0, tokens // block, norm_rows, 0)
    run(fill_chunk, 0)
    run(mixer_gate)
    with jax.named_scope("barrier_wait"):
        pl.semaphore_wait(barrier, n_ep - 1 + 3)
    halo_send()
    run(send_chunk, 0)
    run(w_start)
    for k in range(1, n_chunks):
        run(fill_chunk, k)
    keep_own()
    loads[9].wait()
    turn = lax.broadcasted_iota(jnp.int32, (128, tokens), 0)
    table = jnp.where(turn == 0, slot0r, jnp.where(turn == 1, slot1r, 0.0))
    table = jnp.where(turn == 2, route_t[0:1, :], table)
    table = jnp.where(turn == 3, route_t[1:2, :], table)
    columns = table.T

    loads[10].wait()
    loads[11].wait()
    total[...] = jnp.zeros_like(total)
    run(send_chunk, 1)
    run(send_chunk, 2)
    run(mixer_conv)
    run(w_forward)
    run(wait_in, 0)
    run(gather_start, 0)
    run(mixer_out)
    run(w_along_y)
    for load in loads[4:7]:
        load.wait()
    run(gather_forward, 0)
    run(send_chunk, 3)
    run(wait_in, 1)
    run(gather_start, 1)
    run(gather_done, 0)
    run(compute, 0)
    run(gather_forward, 1)
    run(wait_in, 2)
    run(gather_start, 2)
    run(gather_done, 1)
    run(compute, 1)
    run(gather_forward, 2)
    run(scatter_add, 1)
    run(w_forward_y)
    run(gather_done, 2)
    run(compute, 2)
    run(wait_in, 3)
    run(compute, 3)
    run(give_back, 1)
    run(scatter_add, 2)
    run(scatter_add, 3)
    run(w_share)
    run(give_back, 2)
    run(scatter_add, 0)
    run(give_back, 3)
    run(combine, 1)
    run(give_back, 0)
    run(mixer_project)
    for k in range(n_chunks):
        w0, wn, g0, gn = parts_of(k)
        if wn:
            region = send_full.at[:, pl.ds(0, wn - less_own(k, True)), :]
            rdma(region, region, A2A_S, A2A_R, k, ep, xp).wait_send()
        if gn:
            region = send_part.at[pl.ds(0, gn - less_own(k, False)), :]
            rdma(region, region, A2P_S, A2P_R, k, ep, xp).wait_send()
            region = xin.at[x, pl.ds(g0, gn), :]
            rdma(region, region, AGR_S, AGR_R, k, ep, xp).wait_send()
            rdma(region, region, AGL_S, AGL_R, k, ep, xm).wait_send()
            region = xin.at[x, pl.ds(g0, gn // 2), :]
            rdma(region, region, FWR_S, FWR_R, k, ep, xp).wait_send()
            rdma(region, region, FWL_S, FWL_R, k, ep, xm).wait_send()
        rdma(s1r.at[k], s1r.at[k], S1R_S, S1R_R, k, ep, xp).wait_send()
        rdma(s1l.at[k], s1l.at[k], S1L_S, S1L_R, k, ep, xm).wait_send()
        rdma(s2r.at[k], s2r.at[k], S2R_S, S2R_R, k, ep, xp).wait_send()
        rdma(s2l.at[k], s2l.at[k], S2L_S, S2L_R, k, ep, xm).wait_send()
    mcopy(tail, tail, HALO, ep, xp).wait_send()
    for row in (STAT_P, STAT_M, STAT_O):
        mcopy(stat, stat, row, ep, xp).wait_send()
    for row in (ACT_P, ACT_M, ACT_O):
        mcopy(act_in.at[0], act_in.at[0], row, ep, xp).wait_send()
    sent = w_out.at[x, yy, core]
    mcopy(sent, sent, WR, ep, xp).wait_send()
    mcopy(sent, sent, WL, ep, xp).wait_send()
    sent = w_out.at[x, yy, core, pl.ds(0, w_rows // 2), :]
    mcopy(sent, sent, WFR, ep, xp).wait_send()
    mcopy(sent, sent, WFL, ep, xp).wait_send()
    if ny > 1:
        sent = w_out.at[pl.ds(0, 3), yy, core]
        mcopy(sent, sent, YR, y_up, x).wait_send()
        mcopy(sent, sent, YL, y_down, x).wait_send()
        sent = w_out.at[pl.ds(0, 3), yy, core, pl.ds(0, w_rows // 2), :]
        mcopy(sent, sent, YFR, y_up, x).wait_send()
        mcopy(sent, sent, YFL, y_down, x).wait_send()
    sent = w_out.at[pl.ds(0, 3), :, core]
    mcopy(sent, sent, WC, partner, x).wait_send()
    run(combine, 2)
    run(combine, 3)
    run(combine, 0)
    out[...] = total[...].astype(BF16)
    for k in range(n_chunks):
        back = ans.at[pl.ds(k * rows, rows - less_own(k, bool(whole[own]))), :]
        rdma(back, back, RET_S, RET_R, k, ep, xp).wait_send()


def on_device(
    glu_value,
    glu_gate,
    conv_kernel,
    ln_gain,
    out_weight,
    moe_input,
    moe_gain,
    gate_weight,
    up_weight,
    down_weight,
    expert_ids,
    route_weight,
):
    tokens, width = moe_input.shape
    length, channels_dev = glu_value.shape
    ep_count = lax.axis_size("ep")
    nyc, order, whole, per_chunk = layout_of(ep_count)
    nz = ep_count // nyc
    cap = 16
    hidden_dev = gate_weight.shape[2]
    quarter = width // 4
    n_chunks = nz // per_chunk
    rows = per_chunk * nyc * cap
    slots = ep_count * cap
    vmem = pl.BlockSpec(memory_space=pltpu.VMEM)
    hbm = pl.BlockSpec(memory_space=pl.ANY)
    n_whole = sum(whole) * nyc * cap
    cfg = (nz, nyc, order, whole, per_chunk, cap)
    return pl.pallas_call(
        functools.partial(block_kernel, cfg),
        out_shape=(
            pltpu.VMEM((length // 4, width), BF16),
            pltpu.VMEM((tokens, quarter), BF16),
        ),
        in_specs=[hbm] * 12,
        out_specs=(vmem, vmem),
        scratch_shapes=[
            pltpu.VMEM((1, width), F32),
            pltpu.VMEM(expert_ids.shape[::-1], jnp.int32),
            pltpu.VMEM(route_weight.shape[::-1], F32),
            pltpu.VMEM(conv_kernel.shape, F32),
            pltpu.VMEM((1, channels_dev), F32),
            pltpu.VMEM((tokens, width), BF16),
            pltpu.VMEM((length, channels_dev), BF16),
            pltpu.VMEM((length, channels_dev), BF16),
            pltpu.VMEM((4, nyc // 2, 2, channels_dev // nyc, width), BF16),
            pltpu.VMEM((width, hidden_dev), BF16),
            pltpu.VMEM((width, hidden_dev), BF16),
            pltpu.VMEM((hidden_dev, width), BF16),
            pltpu.VMEM((4, tokens, quarter), BF16),
            pltpu.VMEM((4, max(n_whole, 16), quarter), BF16),
            pltpu.VMEM((max(slots - n_whole, 16), quarter), BF16),
            pltpu.VMEM((4, slots, quarter), BF16),
            pltpu.VMEM((rows, hidden_dev), BF16),
            pltpu.VMEM((n_chunks, 4, rows, quarter), BF16),
            pltpu.VMEM((n_chunks, rows // 2, quarter), BF16),
            pltpu.VMEM((n_chunks, rows // 2, quarter), BF16),
            pltpu.VMEM((n_chunks, rows, quarter), BF16),
            pltpu.VMEM((n_chunks, rows, quarter), BF16),
            pltpu.VMEM((slots, quarter), BF16),
            pltpu.VMEM((slots, quarter), BF16),
            pltpu.VMEM((32, channels_dev), BF16),
            pltpu.VMEM((32, channels_dev), BF16),
            pltpu.VMEM((channels_dev // 128, length + 32, 128), F32),
            pltpu.VMEM((length, channels_dev), F32),
            pltpu.VMEM((8, length), F32),
            pltpu.VMEM((3, 8, length), F32),
            pltpu.VMEM((length, channels_dev), BF16),
            pltpu.VMEM((4, length // 4, channels_dev), BF16),
            pltpu.VMEM((tokens, quarter), F32),
            pltpu.SemaphoreType.DMA((12,)),
            pltpu.SemaphoreType.DMA((22, n_chunks)),
            pltpu.SemaphoreType.DMA((16,)),
            pltpu.SemaphoreType.DMA((16,)),
        ],
        compiler_params=pltpu.CompilerParams(
            collective_id=0, has_side_effects=True, vmem_limit_bytes=60 * 1024 * 1024
        ),
        name="block",
    )(
        moe_gain[None, :],
        expert_ids.T,
        route_weight.T,
        conv_kernel,
        ln_gain[None, :],
        moe_input,
        glu_value,
        glu_gate,
        out_weight.reshape(nyc // 2, 2, channels_dev // nyc, width),
        gate_weight,
        up_weight,
        down_weight,
    )


def solution(mesh):
    in_specs = (
        P("ep", "tp"),
        P("ep", "tp"),
        P(None, "tp"),
        P("tp"),
        P("tp", None),
        P("ep", None),
        P(),
        P("ep", None, "tp"),
        P("ep", None, "tp"),
        P("ep", "tp", None),
        P("ep", None),
        P("ep", None),
    )
    out_specs = (P(("ep", "tp"), None), P("ep", "tp"))
    return jax.shard_map(
        on_device, mesh=mesh, in_specs=in_specs, out_specs=out_specs, check_vma=False
    )
```
